128 devices in a mesh: ep: 16 (over z, x), tp: 8 (over y, core).
Axes of the slice: x: 4, y: 4, z: 4, core: 2. Of those that a mesh axis runs over, the one named last changes fastest.
Arguments:
- query_latent: bfloat16 [16384, 768], P(('ep', 'tp')), may hold values from -6 to 6
- kv_latent: bfloat16 [16384, 512], P(('ep', 'tp')), may hold values from -6 to 6
- rope_key: bfloat16 [16384, 64], P(('ep', 'tp')), may hold values from -6 to 6
- query_gain: float32 [768], replicated, may hold values from 0.1 to 12
- kv_gain: float32 [512], replicated, may hold values from 0.1 to 12
- query_nope_w: bfloat16 [768, 1024], P(None, 'tp'), may hold values from -0.21875 to 0.21875
- query_rope_w: bfloat16 [768, 512], P(None, 'tp'), may hold values from -0.21875 to 0.21875
- key_up_w: bfloat16 [512, 1024], P(None, 'tp'), may hold values from -0.25 to 0.25
- value_up_w: bfloat16 [512, 1024], P(None, 'tp'), may hold values from -0.25 to 0.25
- output_w: bfloat16 [1024, 2048], P('tp'), may hold values from -0.1875 to 0.1875
- expert_in: bfloat16 [16384, 2048], P(('ep', 'tp')), may hold values from -6 to 6
- moe_gain: float32 [2048], replicated, may hold values from 0.1 to 12
- routes: int32 [16384, 2], P(('ep', 'tp')), may hold values from 0 to 31, all different within a row; in each aligned block of 128 rows (0 to 127, 128 to 255, ...) at most 10 rows name the same one
- route_weight: float32 [16384, 2], P(('ep', 'tp')), may hold values from 0.1 to 1
- gate_w: bfloat16 [32, 2048, 2048], P('ep', None, 'tp'), may hold values from -0.125 to 0.125
- up_w: bfloat16 [32, 2048, 2048], P('ep', None, 'tp'), may hold values from -0.125 to 0.125
- down_w: bfloat16 [32, 2048, 2048], P('ep', 'tp'), may hold values from -0.125 to 0.125
Outputs:
- mixer_out: bfloat16 [16384, 2048], P(('ep', 'tp'))
- expert_out: bfloat16 [16384, 2048], P(('ep', 'tp'))
The draws below stay inside these ranges and needn't reach their ends.
Inputs may be any that keep to these rules, and one draw needn't show every extreme that they name: `routes`: each row names 2 different experts; in the rows of one device no expert is named more than 10 times.
All inputs are finite; a program needn't handle non-finite values.
Results may differ from the reference program's by a relative error of at most 0.015.
The reference program's roundings to bfloat16 on the way count: a program that leaves them out, or rounds other values in their place, can miss the bound.
Values may be sent and summed in bfloat16 or wider, within the bound.
No kernel may reach another device: no remote copies, remote signals or barrier semaphores. Data moves between devices by JAX's collectives and lax.ppermute only.
A program may use at most 128 MiB of HBM per device.

```python
import math
import jax
import jax.numpy as jnp
import numpy as np
from jax import lax

D = 2048
HEADS = 8
NOPE = 128
ROPE = 64
VDIM = 128
QLAT = 768
KVLAT = 512
FF = 2048
TOPK = 2
TOK_B = 128
EXPERTS = 32
CAP = 10
TOKENS_A = 16384
TOKENS_B = 16384
N_EP = 16
N_TP = 8


def gain_draw(key, count):
    return 1.0 + 0.18 * jnp.clip(jax.random.normal(key, (count,), jnp.float32), -5.0, 5.0)


def draw_query_gain(key, part):
    return gain_draw(jax.random.fold_in(key, 11), QLAT)


def draw_kv_gain(key, part):
    return gain_draw(jax.random.fold_in(key, 23), KVLAT)


def draw_moe_gain(key, part):
    return gain_draw(jax.random.fold_in(key, 37), D)


def levels(rng, dims, shards, low, top_value):
    loudness, own = 1.0, jax.random.fold_in(rng, 6)
    for position, blocks in shards:
        heights = jnp.exp(jax.random.uniform(jax.random.fold_in(own, position), (blocks,), jnp.float32, low / len(shards), top_value / len(shards)))
        loudness = loudness * jnp.repeat(heights, dims[position] // blocks).reshape([-1 if axis == position else 1 for axis in range(len(dims))])
    return loudness


def assign_block(own_key, own, number, rows, number_of, top, bound, skew):
    ranking = jax.random.permutation(own_key, number_of)
    packed, common = load_shares(number_of, rows * top, bound, skew, True), load_shares(number_of, rows * top, bound, skew, False)
    places = jnp.arange(number_of)

    def named(lengths, offset_by):
        used = int((lengths > 0).sum())
        fixed = max(1, used // 4)
        shifted = fixed + (places - fixed + offset_by * (used - fixed)) % max(1, number_of - fixed)
        return jnp.zeros((number_of,), jnp.int32).at[ranking[jnp.where(places < fixed, places, shifted)]].set(jnp.asarray(lengths, jnp.int32))

    lengths = jnp.where(number % 4 == 0, named(packed, number // 4), named(common, number - number // 4 - 1))
    mixed = jax.random.permutation(jax.random.fold_in(own, 3), number_of)
    donor, receiver = mixed[0:number_of // 2 * 2:2], mixed[1:number_of // 2 * 2:2]
    room = jnp.minimum(lengths[donor] - 1, bound - lengths[receiver]) // 2
    room = jnp.where((donor == ranking[0]) | (receiver == ranking[0]) | (lengths[receiver] == 0), 0, jnp.maximum(room, 0))
    shifted = jax.random.randint(jax.random.fold_in(own, 4), (number_of // 2,), 0, 1 << 20) % (room + 1)
    lengths = lengths.at[donor].add(-shifted).at[receiver].add(shifted)
    members = jnp.searchsorted(jnp.cumsum(lengths), jnp.arange(rows * top), side="right").astype(jnp.int32)
    listing = members.reshape(top, rows).T
    listing = listing[jax.random.permutation(jax.random.fold_in(own, 1), rows)]
    offset_by = jax.random.randint(jax.random.fold_in(own, 2), (rows, 1), 0, top)
    return jnp.take_along_axis(listing, (jnp.arange(top)[None, :] + offset_by) % top, axis=1)


def load_shares(count, total, bound, slope, full):
    weights = [(1 << 20) // math.isqrt(rank ** slope) + 1 for rank in range(1, count + 1)]
    largest = bound if full else min(bound, max(-(-total // count), total * weights[0] // sum(weights)))
    least = 1 if total - largest >= count - 1 else 0
    given, surplus = [largest] + [least] * (count - 1), total - largest - least * (count - 1)
    while surplus > 0:
        candidates = [i for i in range(1, count) if given[i] < largest] or [i for i in range(1, count) if given[i] < bound]
        pool, budget = sum([weights[i] for i in candidates]), surplus
        for i in candidates:
            extra = min(bound - given[i], max(1, budget * weights[i] // pool), surplus)
            given[i] = given[i] + extra
            surplus = surplus - extra
    return np.array(given)


def noise(stream_key, shape, scale, reach, shards=(), kind=jnp.bfloat16):
    entries = scale * jax.random.normal(stream_key, shape, jnp.float32)
    if shards:
        entries = entries * levels(stream_key, shape, shards, -0.22, 0.18)
    return jnp.clip(entries, -reach, reach).astype(kind)


def setup_inputs(seed: int = 0) -> dict:
    key_list = jax.random.split(jax.random.key(seed), 18)
    query_latent = noise(key_list[0], (TOKENS_A, QLAT), 1.0, 6.0, ((0, 128),))
    kv_latent = noise(key_list[1], (TOKENS_A, KVLAT), 1.0, 6.0, ((0, 128),))
    rope_key = noise(key_list[2], (TOKENS_A, ROPE), 1.0, 6.0, ((0, 128),))
    query_gain = draw_query_gain(jax.random.fold_in(key_list[17], 71), 0)
    kv_gain = draw_kv_gain(jax.random.fold_in(key_list[17], 71), 0)
    query_nope_w = noise(key_list[5], (QLAT, HEADS * NOPE), QLAT ** -0.5, 0.21875, ((1, 8),))
    query_rope_w = noise(key_list[6], (QLAT, HEADS * ROPE), QLAT ** -0.5, 0.21875, ((1, 8),))
    key_up_w = noise(key_list[7], (KVLAT, HEADS * NOPE), KVLAT ** -0.5, 0.25, ((1, 8),))
    value_up_w = noise(key_list[8], (KVLAT, HEADS * VDIM), KVLAT ** -0.5, 0.25, ((1, 8),))
    output_w = noise(key_list[9], (HEADS * VDIM, D), (HEADS * VDIM) ** -0.5, 0.1875, ((0, 8),))
    expert_in = noise(key_list[10], (TOKENS_B, D), 1.0, 6.0, ((0, 128),))
    moe_gain = draw_moe_gain(jax.random.fold_in(key_list[17], 71), 0)
    routes_keys = jax.random.split(jax.random.fold_in(key_list[12], 1), TOKENS_B // TOK_B)
    routes_turns = jax.random.permutation(jax.random.fold_in(key_list[12], 3), TOKENS_B // TOK_B)
    routes = jax.vmap(lambda own, number: assign_block(jax.random.fold_in(key_list[12], 2), own, number, TOK_B, EXPERTS, TOPK, CAP, 1))(routes_keys, routes_turns).reshape((TOKENS_B, TOPK))
    route_weight = jnp.clip(jnp.exp(math.log(1.0) - 2.3025851 * jax.random.uniform(key_list[13], (TOKENS_B, TOPK), jnp.float32) ** levels(key_list[13], (TOKENS_B, TOPK), ((0, 128),), -0.2, 0.2)), 0.1, 1.0)
    gate_w = noise(key_list[14], (EXPERTS, D, FF), D ** -0.5, 0.125, ((0, 16), (2, 8)))
    up_w = noise(key_list[15], (EXPERTS, D, FF), D ** -0.5, 0.125, ((0, 16), (2, 8)))
    down_w = noise(key_list[16], (EXPERTS, FF, D), FF ** -0.5, 0.125, ((0, 16), (1, 8)))
    return dict(query_latent=query_latent, kv_latent=kv_latent, rope_key=rope_key, query_gain=query_gain, kv_gain=kv_gain, query_nope_w=query_nope_w, query_rope_w=query_rope_w, key_up_w=key_up_w, value_up_w=value_up_w, output_w=output_w, expert_in=expert_in, moe_gain=moe_gain, routes=routes, route_weight=route_weight, gate_w=gate_w, up_w=up_w, down_w=down_w)


THETA = 10000.0

def rms_scale(values, gain):
    floats = values.astype(jnp.float32)
    square = lax.optimization_barrier(jnp.mean(floats * floats, axis=-1, keepdims=True))
    return (floats * lax.rsqrt(square + 1e-06) * gain).astype(jnp.bfloat16)

def rotate(values, positions):
    width = values.shape[-1]
    half = width // 2
    freq = 1.0 / THETA ** (jnp.arange(half, dtype=jnp.float32) * 2.0 / width)
    angle = positions.astype(jnp.float32)[:, None] * freq[None, :]
    angle = jnp.concatenate([angle, angle], axis=-1)
    cosine = jnp.cos(angle)
    sine = jnp.sin(angle)
    if values.ndim == 3:
        cosine = cosine[:, None, :]
        sine = sine[:, None, :]
    first = values[..., :half]
    second = values[..., half:]
    turned = jnp.concatenate([-second, first], axis=-1)
    return values * cosine + turned * sine

def expert_rows(rows, gate_one, up_one, down_one):
    gate = jnp.minimum(jnp.dot(rows, gate_one, preferred_element_type=jnp.float32), 7.0)
    upper = jnp.clip(jnp.dot(rows, up_one, preferred_element_type=jnp.float32), -7.0, 7.0)
    hidden = (gate * jax.nn.sigmoid(1.702 * gate) * (upper + 1.0)).astype(jnp.bfloat16)
    count = rows.shape[0]
    slices = hidden.reshape(count, N_TP, FF // N_TP).astype(jnp.float32)
    downs = down_one.reshape(N_TP, FF // N_TP, D).astype(jnp.float32)
    parts = jnp.einsum('rsf,sfd->srd', slices, downs)
    parts = lax.optimization_barrier(parts.astype(jnp.bfloat16)).astype(jnp.float32)
    return lax.optimization_barrier(jnp.sum(parts, axis=0)).astype(jnp.bfloat16)

def reference(query_latent, kv_latent, rope_key, query_gain, kv_gain, query_nope_w, query_rope_w, key_up_w, value_up_w, output_w, expert_in, moe_gain, routes, route_weight, gate_w, up_w, down_w):
    length = query_latent.shape[0]
    positions = jnp.arange(length, dtype=jnp.int32)
    query_normed = rms_scale(query_latent, query_gain)
    kv_normed = rms_scale(kv_latent, kv_gain)
    query_flat = jnp.dot(query_normed, query_nope_w, preferred_element_type=jnp.float32).astype(jnp.bfloat16)
    key_flat = jnp.dot(kv_normed, key_up_w, preferred_element_type=jnp.float32).astype(jnp.bfloat16)
    value_flat = jnp.dot(kv_normed, value_up_w, preferred_element_type=jnp.float32).astype(jnp.bfloat16)
    query_turn = jnp.dot(query_normed, query_rope_w, preferred_element_type=jnp.float32).reshape(length, HEADS, ROPE)
    query_rot = rotate(query_turn, positions).astype(jnp.bfloat16)
    key_rot = rotate(rope_key.astype(jnp.float32), positions).astype(jnp.bfloat16)
    queries = jnp.concatenate([query_flat.reshape(length, HEADS, NOPE), query_rot], axis=-1).astype(jnp.float32)
    keys = jnp.concatenate([key_flat.reshape(length, HEADS, NOPE), jnp.broadcast_to(key_rot[:, None, :], (length, HEADS, ROPE))], axis=-1).astype(jnp.float32)
    values = value_flat.reshape(length, HEADS, VDIM).astype(jnp.float32)
    block = math.gcd(length, 512)
    scale = 1.0 / math.sqrt(NOPE + ROPE)

    def attend(start):
        query_block = lax.dynamic_slice_in_dim(queries, start, block, 0)
        scores = jnp.einsum('qhd,khd->hqk', query_block, keys) * scale
        allowed = positions[None, :] <= (start + jnp.arange(block, dtype=jnp.int32))[:, None]
        masked = jnp.where(allowed[None], scores, -1e+30)
        peak = lax.optimization_barrier(jnp.max(masked, axis=-1, keepdims=True))
        expo = jnp.where(allowed[None], jnp.exp(masked - peak), 0.0)
        total = lax.optimization_barrier(jnp.sum(expo, axis=-1))
        probs = expo.astype(jnp.bfloat16).astype(jnp.float32)
        summed = jnp.einsum('hqk,khd->qhd', probs, values)
        return (summed / jnp.transpose(total)[:, :, None]).astype(jnp.bfloat16)
    starts = jnp.arange(length // block, dtype=jnp.int32) * block
    attended = lax.map(attend, starts).reshape(length, HEADS * VDIM)
    group = HEADS * VDIM // N_TP
    mixed = jnp.zeros((length, D), jnp.float32)
    for index in range(N_TP):
        part = jnp.dot(attended[:, index * group:(index + 1) * group], output_w[index * group:(index + 1) * group], preferred_element_type=jnp.float32)
        mixed = mixed + lax.optimization_barrier(part.astype(jnp.bfloat16)).astype(jnp.float32)
    mixer_out = mixed.astype(jnp.bfloat16)
    floats = expert_in.astype(jnp.float32)
    center = floats - lax.optimization_barrier(jnp.mean(floats, axis=-1, keepdims=True))
    variance = lax.optimization_barrier(jnp.mean(center * center, axis=-1, keepdims=True))
    normed_in = (center * lax.rsqrt(variance + 1e-05) * moe_gain).astype(jnp.bfloat16)
    tokens_b = expert_in.shape[0]
    flat = routes.reshape(-1).astype(jnp.int32)
    assigned = flat.shape[0]
    owner = (jnp.arange(assigned, dtype=jnp.int32) // TOPK).astype(jnp.int32)
    weights = route_weight / lax.optimization_barrier(jnp.sum(route_weight, axis=-1, keepdims=True))
    flat_weight = weights.reshape(-1)
    order = jnp.argsort(flat, stable=True).astype(jnp.int32)
    counts = lax.optimization_barrier(jnp.sum((flat[:, None] == jnp.arange(EXPERTS, dtype=jnp.int32)[None, :]).astype(jnp.int32), axis=0))
    firsts = (jnp.cumsum(counts) - counts).astype(jnp.int32)
    most_rows = N_EP * N_TP * CAP

    def per_expert(total, expert):
        offsets = jnp.arange(most_rows, dtype=jnp.int32)
        valid = offsets < counts[expert]
        index = jnp.minimum(firsts[expert] + offsets, assigned - 1).astype(jnp.int32)
        picked = order[index]
        rows = normed_in[owner[picked]]
        result = expert_rows(rows, gate_w[expert], up_w[expert], down_w[expert])
        factor = jnp.where(valid, flat_weight[picked], 0.0)
        total = total.at[owner[picked]].add(factor[:, None] * result.astype(jnp.float32))
        return (total, None)
    combined, unused = lax.scan(per_expert, jnp.zeros((tokens_b, D), jnp.float32), jnp.arange(EXPERTS, dtype=jnp.int32))
    return (mixer_out, combined.astype(jnp.bfloat16))
```

```python
import functools
import math

import jax
import jax.numpy as jnp
import numpy as np
from jax import lax
from jax.experimental import pallas as pl
from jax.experimental.pallas import tpu as pltpu
from jax.sharding import PartitionSpec as P


NOPE = 128
ROPE = 64
VDIM = 128
THETA = 10000.0
CHUNK = 24
HALF = 12
CAP = 10
BF = jnp.bfloat16
F32 = jnp.float32
LOG2E = 1.4426950408889634


def dot(a, b, dims=(((1,), (0,)), ((), ()))):
    return lax.dot_general(a, b, dims, preferred_element_type=F32)


def shift_z(d):
    return [(e, ((e // 4 + d) % 4) * 4 + e % 4) for e in range(16)]


def shift_x(d):
    return [(e, (e // 4) * 4 + (e % 4 + d) % 4) for e in range(16)]


def shift_y(d):
    return [(t, ((t // 2 + d) % 4) * 2 + t % 2) for t in range(8)]


SWAP = [(t, t ^ 1) for t in range(8)]


def send_z(a, d):
    return lax.ppermute(a, "ep", shift_z(d))


def send_x(a, d):
    return lax.ppermute(a, "ep", shift_x(d))


def send_y(a, d):
    return lax.ppermute(a, "tp", shift_y(d))


def swap(a):
    return lax.ppermute(a, "tp", SWAP)


def ring(one, two, send):
    one_below = send(one, 1)
    two_above = send(two, -1)
    two_below = send(two, 1)
    one_above = send(one, -1)
    one_far = send(one_below, 1)
    two_far = send(two_above, -1)
    return (one_below, two_below), (one_above, two_above), (one_far, two_far)


def slots_of(route, rank):
    return (route >> 1) * CHUNK + (route & 1) * HALF + rank


def dispatch_body(x_ref, gain_ref, col_ref, row_ref, after_ref, out_ref):
    floats = x_ref[...].astype(F32)
    center = floats - jnp.mean(floats, axis=-1, keepdims=True)
    variance = jnp.mean(center * center, axis=-1, keepdims=True)
    normed = (center * lax.rsqrt(variance + 1e-05) * gain_ref[...]).astype(BF)
    count = x_ref.shape[0]
    j = lax.broadcasted_iota(jnp.int32, (count, count), 0)
    i = lax.broadcasted_iota(jnp.int32, (count, count), 1)
    earlier = j < i
    total = out_ref.shape[0]
    number = lax.broadcasted_iota(jnp.int32, (total, count), 0)
    select = None
    for k in range(2):
        mine = row_ref[k : k + 1, :]
        same = (col_ref[:, 0:1] == mine) | (col_ref[:, 1:2] == mine)
        rank = jnp.sum(jnp.where(same & earlier, 1.0, 0.0), axis=0, keepdims=True)
        hit = number == slots_of(mine, rank.astype(jnp.int32))
        select = hit if select is None else select | hit
    pick = jnp.where(select, 1.0, 0.0).astype(BF)
    out_ref[...] = dot(pick, normed).astype(BF)


def dispatch(x, gain, routes, after):
    vmem = pl.BlockSpec(memory_space=pltpu.VMEM)
    return pl.pallas_call(
        dispatch_body,
        in_specs=[vmem] * 4 + [pl.BlockSpec(memory_space=pl.ANY)],
        out_specs=vmem,
        out_shape=jax.ShapeDtypeStruct((16 * CHUNK, x.shape[1]), BF),
        name="dispatch",
    )(x, gain.reshape(1, -1), routes, routes.T, after)


def combine_body(back_ref, col_ref, row_ref, w_ref, out_ref):
    count = col_ref.shape[0]
    i = lax.broadcasted_iota(jnp.int32, (count, count), 0)
    j = lax.broadcasted_iota(jnp.int32, (count, count), 1)
    earlier = j < i
    total = back_ref.shape[0]
    number = lax.broadcasted_iota(jnp.int32, (count, total), 1)
    weight = w_ref[...]
    weight = weight / jnp.sum(weight, axis=-1, keepdims=True)
    back = back_ref[...]
    result = None
    for k in range(2):
        mine = col_ref[:, k : k + 1]
        same = (row_ref[0:1, :] == mine) | (row_ref[1:2, :] == mine)
        rank = jnp.sum(jnp.where(same & earlier, 1.0, 0.0), axis=1, keepdims=True)
        hit = number == slots_of(mine, rank.astype(jnp.int32))
        pick = jnp.where(hit, 1.0, 0.0).astype(BF)
        term = dot(pick, back) * weight[:, k : k + 1]
        result = term if result is None else result + term
    out_ref[...] = result.astype(BF)


def combine(back, routes, route_weight):
    return pl.pallas_call(
        combine_body,
        out_shape=jax.ShapeDtypeStruct((routes.shape[0], back.shape[1]), BF),
        name="combine",
    )(back, routes, routes.T, route_weight)


def packing():
    rows, cols = 16 * 2 * CAP, 16 * CHUNK
    r = lax.broadcasted_iota(jnp.int32, (rows, cols), 0)
    c = lax.broadcasted_iota(jnp.int32, (rows, cols), 1)
    per = 16 * CAP
    slot = ((r % per) // CAP) * CHUNK + (r // per) * HALF + r % CAP
    return (slot == c).astype(BF)


def pack_body(pick_ref, x_ref, one_ref, two_ref):
    rows = one_ref.shape[0]
    packed = dot(pick_ref[...], x_ref[...]).astype(BF)
    one_ref[...] = packed[:rows]
    two_ref[...] = packed[rows:]


def pack(pick, arrived):
    out = jax.ShapeDtypeStruct((pick.shape[0] // 2, arrived.shape[1]), BF)
    return pl.pallas_call(pack_body, out_shape=[out, out], name="pack")(pick, arrived)


def unpack_body(pick_ref, *refs):
    out_ref = refs[-1]
    one = refs[0][...].astype(F32) + refs[1][...].astype(F32) + refs[2][...].astype(F32)
    two = refs[3][...].astype(F32) + refs[4][...].astype(F32) + refs[5][...].astype(F32)
    summed = jnp.concatenate([one.astype(BF), two.astype(BF)], axis=0)
    out_ref[...] = dot(pick_ref[...], summed, (((0,), (0,)), ((), ()))).astype(BF)


def unpack(pick, *terms):
    out = jax.ShapeDtypeStruct((pick.shape[1], terms[0].shape[1]), BF)
    return pl.pallas_call(unpack_body, out_shape=out, name="unpack")(pick, *terms)


def ffn_body(count, expert, *refs):
    xs = refs[:count]
    sources = refs[count : count + 6]
    outs = refs[count + 6 : 2 * count + 6]
    gates, uppers, downs, sems = refs[2 * count + 6 :]
    copies = []
    for half in range(2):
        for k, target in enumerate((gates, uppers, downs)):
            number = half * 3 + k
            copies.append(
                pltpu.make_async_copy(sources[number].at[expert], target.at[half], sems.at[number])
            )
    for copy in copies:
        copy.start()
    x = xs[0][...] if count == 1 else jnp.concatenate([r[...] for r in xs], axis=0)
    whole = None
    for half in range(2):
        copies[half * 3].wait()
        gate = jnp.minimum(dot(x, gates[half]), 7.0)
        copies[half * 3 + 1].wait()
        upper = jnp.clip(dot(x, uppers[half]), -7.0, 7.0)
        hidden = (gate * jax.nn.sigmoid(1.702 * gate) * (upper + 1.0)).astype(BF)
        copies[half * 3 + 2].wait()
        part = dot(hidden, downs[half])
        whole = part if whole is None else whole + part
    whole = whole.astype(BF)
    rows = whole.shape[0] // count
    for k in range(count):
        outs[k][...] = whole[k * rows : (k + 1) * rows]


def ffn(xs, expert, weights):
    rows, width = xs[0].shape
    count = len(xs)
    inner = weights[0].shape[2]
    vmem = pl.BlockSpec(memory_space=pltpu.VMEM)
    out = jax.ShapeDtypeStruct((rows, width), BF)
    return pl.pallas_call(
        functools.partial(ffn_body, count, expert),
        in_specs=[vmem] * count + [pl.BlockSpec(memory_space=pl.ANY)] * 6,
        out_specs=[vmem] * count,
        out_shape=[out] * count,
        scratch_shapes=[
            pltpu.VMEM((2, width, inner), BF),
            pltpu.VMEM((2, width, inner), BF),
            pltpu.VMEM((2, inner, width), BF),
            pltpu.SemaphoreType.DMA((6,)),
        ],
        cost_estimate=pl.CostEstimate(
            flops=6 * rows * count * width * 512, bytes_accessed=8 << 20, transcendentals=0
        ),
        name="ffn",
    )(*xs, *weights)


def experts_half(
    expert_in, moe_gain, routes, route_weight, gate_w, up_w, down_w, after
):
    width = expert_in.shape[1]
    outgoing = dispatch(expert_in, moe_gain, routes, after)
    weights = (gate_w, up_w, down_w, swap(gate_w), swap(up_w), swap(down_w))
    arrived = lax.all_to_all(
        outgoing.reshape(16, CHUNK, width), "ep", split_axis=0, concat_axis=0, tiled=True
    ).reshape(16 * CHUNK, width)
    pick = packing()
    one, two = pack(pick, arrived)
    below, above, far = ring(one, two, send_y)
    (own0,) = ffn([one], 0, weights)
    (own1,) = ffn([two], 1, weights)
    below0, above0 = ffn([below[0], above[0]], 0, weights)
    below1, above1 = ffn([below[1], above[1]], 1, weights)
    above1_sent = send_y(above1, 1)
    below0_sent = send_y(below0, -1)
    (far0,) = ffn([far[0]], 0, weights)
    far0_sent = send_y(far0, 1)
    (far1,) = ffn([far[1]], 1, weights)
    far1_sent = send_y(far1, -1)
    above0_sum = (above0.astype(F32) + far0_sent.astype(F32)).astype(BF)
    above0_sent = send_y(above0_sum, 1)
    below1_sum = (below1.astype(F32) + far1_sent.astype(F32)).astype(BF)
    below1_sent = send_y(below1_sum, -1)
    back = unpack(pick, own0, below0_sent, above0_sent, own1, below1_sent, above1_sent)
    back = lax.all_to_all(
        back.reshape(16, CHUNK, width), "ep", split_axis=0, concat_axis=0, tiled=True
    ).reshape(16 * CHUNK, width)
    return combine(back, routes, route_weight)


SCALE2 = LOG2E / math.sqrt(NOPE + ROPE)
QLAT = 768
KVLAT = 512
LATENT = 1536
KEYS = 512
PART = 640
PIECE = 2 * PART
NT = (((1,), (1,)), ((), ()))
LIMIT = 2.0**80


def prepare_body(q_ref, kv_ref, rot_ref, qg_ref, kvg_ref, out_ref):
    for ref, gain, at in ((q_ref, qg_ref, 0), (kv_ref, kvg_ref, QLAT)):
        floats = ref[...].astype(F32)
        square = jnp.mean(floats * floats, axis=-1, keepdims=True)
        normed = floats * lax.rsqrt(square + 1e-06) * gain[...]
        out_ref[:, at : at + ref.shape[1]] = normed.astype(BF)
    rot = rot_ref[...]
    both = jnp.concatenate([rot, jnp.zeros_like(rot)], axis=1)
    out_ref[:, QLAT + KVLAT : QLAT + KVLAT + 128] = both
    out_ref[:, QLAT + KVLAT + 128 :] = jnp.zeros((rot.shape[0], 128), BF)


def prepare(query_latent, kv_latent, key_rot, query_gain, kv_gain):
    return pl.pallas_call(
        prepare_body,
        out_shape=jax.ShapeDtypeStruct((query_latent.shape[0], LATENT), BF),
        name="prepare",
    )(query_latent, kv_latent, key_rot, query_gain.reshape(1, -1), kv_gain.reshape(1, -1))


def heads_body(*refs):
    blocks = refs[:8]
    key_ref, value_ref, query_ref, cos_ref, sin_ref = refs[8:13]
    parts = refs[13:17]
    low_ref, high_ref = refs[17:]
    kv = jnp.concatenate([r[:, QLAT : QLAT + KVLAT] for r in blocks], axis=0)
    keys = dot(kv, key_ref[...]).astype(BF)
    values = dot(value_ref[...], kv, NT).astype(BF)
    rots = jnp.concatenate(
        [r[:, QLAT + KVLAT : QLAT + KVLAT + 128] for r in blocks], axis=0
    ).astype(F32)
    for colour in range(2):
        at = colour * KEYS
        one, two = parts[2 * colour], parts[2 * colour + 1]
        half = KEYS // 2
        pair = rots[at : at + half] + pltpu.roll(rots[at + half : at + KEYS], ROPE, 1)
        pair = pair.astype(BF)
        one[:KEYS, :] = keys[at : at + KEYS]
        one[KEYS:, :] = pair[:128]
        two[:128, :] = pair[128:]
        for c in range(4):
            two[128 * (c + 1) : 128 * (c + 2), :] = values[:, at + 128 * c : at + 128 * (c + 1)]
    query_in = jnp.concatenate([r[:, :QLAT] for r in blocks], axis=0)
    query = dot(query_ref[...], query_in, NT)
    first = query[NOPE : NOPE + ROPE // 2]
    second = query[NOPE + ROPE // 2 :]
    cosine = cos_ref[...]
    sine = sin_ref[...]
    rot = jnp.concatenate([first * cosine - second * sine, second * cosine + first * sine], axis=0)
    nope = query[:NOPE].astype(BF)
    rot = rot.astype(BF)
    blank = jnp.zeros_like(rot)
    low_ref[...] = jnp.concatenate([nope, rot, blank], axis=0)
    high_ref[...] = jnp.concatenate([nope, blank, rot], axis=0)


def heads(blocks, key_w, value_w, query_w, cosine, sine):
    rows = 8 * blocks[0].shape[0]
    part = jax.ShapeDtypeStruct((PART, 128), BF)
    query = jax.ShapeDtypeStruct((256, rows), BF)
    return pl.pallas_call(
        heads_body,
        out_shape=[part] * 4 + [query] * 2,
        cost_estimate=pl.CostEstimate(
            flops=2 * rows * (QLAT * 192 + KVLAT * 256), bytes_accessed=6 << 20, transcendentals=0
        ),
        name="heads",
    )(*blocks, key_w, value_w, query_w, cosine, sine)


def join_body(*refs):
    sources, outs = refs[:8], refs[8:]
    for k, source in enumerate(sources):
        outs[k // 4][(k % 4) * PART : (k % 4 + 1) * PART, :] = source[...]


def join(parts):
    out = jax.ShapeDtypeStruct((2 * PIECE, 128), BF)
    return pl.pallas_call(join_body, out_shape=[out] * 2, name="join")(*parts)


def own_body(kpos_ref, qpos_ref, low_ref, high_ref, *refs):
    parts = refs[:4]
    m_ref, l_ref, acc_ref = refs[-3:]
    tile = 256
    half = KEYS // 2
    lefts = []
    values = []
    for colour in range(2):
        one, two = parts[2 * colour], parts[2 * colour + 1]
        pair = jnp.concatenate([one[KEYS:, :], two[:128, :]], axis=0)
        lefts.append(jnp.concatenate([one[:half, :], pair], axis=1))
        lefts.append(jnp.concatenate([one[half:KEYS, :], pair], axis=1))
        values += [two[128 * c : 128 * (c + 1), :] for c in range(1, 5)]
    value = jnp.concatenate(values, axis=1)
    for part in range(low_ref.shape[1] // tile):
        cols = slice(part * tile, (part + 1) * tile)
        scores = []
        for k, left in enumerate(lefts):
            s = dot(left, (high_ref if k % 2 else low_ref)[:, cols])
            allowed = kpos_ref[k * half : (k + 1) * half, :] <= qpos_ref[:, cols]
            scores.append(jnp.where(allowed, s, -1e30))
        peaks = [jnp.max(s, axis=0, keepdims=True) for s in scores]
        m = jnp.maximum(jnp.maximum(peaks[0], peaks[1]), jnp.maximum(peaks[2], peaks[3]))
        base = m * SCALE2
        probs = [jnp.exp2(s * SCALE2 - base) for s in scores]
        sums = [jnp.sum(p, axis=0, keepdims=True) for p in probs]
        m_ref[:, cols] = m
        l_ref[:, cols] = (sums[0] + sums[1]) + (sums[2] + sums[3])
        acc_ref[:, cols] = dot(value, jnp.concatenate([p.astype(BF) for p in probs], axis=0))


def own_attention(low, high, parts, positions, after):
    rows = low.shape[1]
    thin = jax.ShapeDtypeStruct((1, rows), F32)
    vmem = pl.BlockSpec(memory_space=pltpu.VMEM)
    return pl.pallas_call(
        own_body,
        in_specs=[vmem] * 8 + [pl.BlockSpec(memory_space=pl.ANY)] * len(after),
        out_specs=[vmem] * 3,
        out_shape=[thin, thin, jax.ShapeDtypeStruct((VDIM, rows), F32)],
        cost_estimate=pl.CostEstimate(
            flops=2 * rows * rows * 384, bytes_accessed=4 << 20, transcendentals=rows * rows
        ),
        name="own_attention",
    )(positions.reshape(-1, 1), positions.reshape(1, -1), low, high, *parts, *after)


def load_piece(ref, k):
    at = pl.multiple_of(k * PIECE, PIECE)
    half = KEYS // 2
    pair = ref[pl.ds(at + KEYS, half), :]
    left = jnp.concatenate([ref[pl.ds(at, half), :], pair], axis=1)
    right = jnp.concatenate([ref[pl.ds(at + half, half), :], pair], axis=1)
    value = [ref[pl.ds(at + KEYS + half + 128 * c, 128), :] for c in range(4)]
    return left, right, jnp.concatenate(value, axis=1)


def more_body(arrays, first, final, flags_ref, low_ref, high_ref, *refs):
    pieces = refs[:arrays]
    m_in, l_in, acc_in = refs[arrays : arrays + 3]
    if final:
        out_ref, m_ref, l_ref, acc_ref = refs[arrays + 3 :]
    else:
        m_ref, l_ref, acc_ref = refs[arrays + 3 :]
    tile = 256
    tiles = low_ref.shape[1] // tile

    def start():
        m_ref[...] = m_in[...]
        l_ref[...] = l_in[...]
        acc_ref[...] = acc_in[...]

    def score(piece, t):
        cols = slice(t * tile, (t + 1) * tile)
        return dot(piece[0], low_ref[:, cols]), dot(piece[1], high_ref[:, cols])

    def over(step):
        for number, ref in enumerate(pieces):

            def one(k, _, ref=ref, number=number):
                @pl.when(flags_ref[first + 2 * number + k] != 0)
                def _():
                    step(load_piece(ref, k))

                return 0

            lax.fori_loop(0, 2, one, 0)

    def weigh(s, t):
        cols = slice(t * tile, (t + 1) * tile)
        base = m_ref[:, cols] * SCALE2
        p = jnp.exp2(s[0] * SCALE2 - base)
        q = jnp.exp2(s[1] * SCALE2 - base)
        l_ref[:, cols] += jnp.sum(p, axis=0, keepdims=True) + jnp.sum(q, axis=0, keepdims=True)
        return jnp.concatenate([p.astype(BF), q.astype(BF)], axis=0)

    def gather(piece, probs, t):
        cols = slice(t * tile, (t + 1) * tile)
        acc_ref[:, cols] += dot(piece[2], probs)

    def quick(piece):
        s = score(piece, 0)
        before = None
        for t in range(tiles):
            after = score(piece, t + 1) if t + 1 < tiles else None
            if before is not None:
                gather(piece, before, t - 1)
            before = weigh(s, t)
            s = after
        gather(piece, before, tiles - 1)

    def careful(piece):
        def one(t, _):
            cols = pl.ds(pl.multiple_of(t * tile, tile), tile)
            p = dot(piece[0], low_ref[:, cols])
            q = dot(piece[1], high_ref[:, cols])
            before = m_ref[:, cols]
            peak = jnp.maximum(jnp.max(p, axis=0, keepdims=True), jnp.max(q, axis=0, keepdims=True))
            m = jnp.maximum(before, peak)
            alpha = jnp.exp2((before - m) * SCALE2)
            p = jnp.exp2(p * SCALE2 - m * SCALE2)
            q = jnp.exp2(q * SCALE2 - m * SCALE2)
            m_ref[:, cols] = m
            total = jnp.sum(p, axis=0, keepdims=True) + jnp.sum(q, axis=0, keepdims=True)
            l_ref[:, cols] = l_ref[:, cols] * alpha + total
            probs = jnp.concatenate([p.astype(BF), q.astype(BF)], axis=0)
            acc_ref[:, cols] = acc_ref[:, cols] * alpha + dot(piece[2], probs)
            return 0

        lax.fori_loop(0, tiles, one, 0)

    start()
    over(quick)
    safe = jnp.where(l_ref[...] < LIMIT, 0.0, 1.0)

    @pl.when(jnp.max(safe) > 0.0)
    def _():
        start()
        over(careful)

    if final:
        done = (acc_ref[...] / l_ref[...]).astype(BF)
        for b in range(8):
            out_ref[flags_ref[first + 2 * arrays + b]] = done[:, 128 * b : 128 * (b + 1)]


def more_attention(low, high, arrays, flags, first, state, final=False):
    rows = low.shape[1]
    keys = 2 * len(arrays) * KEYS
    shapes = [(1, rows), (1, rows), (VDIM, rows)]
    if final:
        out_shape = jax.ShapeDtypeStruct((8, VDIM, 128), BF)
        scratch = [pltpu.VMEM(s, F32) for s in shapes]
    else:
        out_shape = [jax.ShapeDtypeStruct(s, F32) for s in shapes]
        scratch = []
    vmem = pl.BlockSpec(memory_space=pltpu.VMEM)
    return pl.pallas_call(
        functools.partial(more_body, len(arrays), first, final),
        in_specs=[pl.BlockSpec(memory_space=pltpu.SMEM)] + [vmem] * (5 + len(arrays)),
        out_specs=vmem if final else [vmem] * 3,
        out_shape=out_shape,
        scratch_shapes=scratch,
        cost_estimate=pl.CostEstimate(
            flops=rows * keys * 384, bytes_accessed=4 << 20, transcendentals=rows * keys
        ),
        name="more_attention",
    )(flags, low, high, *arrays, *state)


def project_body(flags_ref, att_ref, *refs):
    out_ref = refs[-1]
    blocks = refs[:-1]
    at = flags_ref.shape[0] - len(blocks)
    left = jnp.concatenate([att_ref[flags_ref[at + j]] for j in range(len(blocks))], axis=0)
    right = jnp.concatenate([b[...] for b in blocks], axis=0)
    out_ref[...] = dot(left, right, (((0,), (0,)), ((), ()))).astype(BF)


def project(att, blocks, flags):
    rows = att.shape[2]
    width = blocks[0].shape[1]
    cols = 512
    return pl.pallas_call(
        project_body,
        grid_spec=pltpu.PrefetchScalarGridSpec(
            num_scalar_prefetch=1,
            grid=(width // cols,),
            in_specs=[pl.BlockSpec(att.shape, lambda n, o: (0, 0, 0))]
            + [pl.BlockSpec((128, cols), lambda n, o: (0, n))] * len(blocks),
            out_specs=pl.BlockSpec((rows, cols), lambda n, o: (0, n)),
        ),
        out_shape=jax.ShapeDtypeStruct((rows, width), BF),
        name="project",
    )(flags, att, *blocks)


def angles(positions):
    half = ROPE // 2
    freq = 1.0 / THETA ** (jnp.arange(half, dtype=F32) * 2.0 / ROPE)
    return positions.astype(F32), freq


def turn(values):
    half = ROPE // 2
    return jnp.concatenate([-values[:, half:], values[:, :half]], axis=-1)


STEPS = (1, -1, 2)
LINE = (0, 1, -1, 2)


def sources():
    near = [(d, 0) for d in LINE] + [(0, d) for d in LINE]
    wide = [(a, b) for b in (1, -1) for a in LINE] + [(b, a) for b in (1, -1) for a in LINE]
    far = [(a, 2) for a in LINE] + [(2, a) for a in LINE]
    return near + wide + far


def own_block(query_latent, kv_latent, rope_key, query_gain, kv_gain):
    local = query_latent.shape[0]
    first = (lax.axis_index("ep") * 8 + lax.axis_index("tp")) * local
    place, freq = angles(first + jnp.arange(local, dtype=jnp.int32))
    angle = place[:, None] * freq[None, :]
    angle = jnp.concatenate([angle, angle], axis=-1)
    key_in = rope_key.astype(F32)
    key_rot = (key_in * jnp.cos(angle) + turn(key_in) * jnp.sin(angle)).astype(BF)
    return prepare(query_latent, kv_latent, key_rot, query_gain, kv_gain)


def mixer(
    query_latent,
    kv_latent,
    rope_key,
    query_gain,
    kv_gain,
    query_nope_w,
    query_rope_w,
    key_up_w,
    value_up_w,
    output_w,
    block,
):
    local = query_latent.shape[0]
    group = local * 8
    ep = lax.axis_index("ep")
    tp = lax.axis_index("tp")
    z, x = ep // 4, ep % 4
    y, core = tp // 2, tp % 2
    below, above, far = ring(block, output_w, send_y)
    gathered = [(block, output_w), below, above, far]
    latents = [a for pair in gathered for a in (pair[0], swap(pair[0]))]
    outputs = [a for pair in gathered for a in (pair[1], swap(pair[1]))]
    chip = np.array([d for d in (0, -1, 1, 2) for c in (0, 1)], np.int32)
    side = np.array([c for d in (0, -1, 1, 2) for c in (0, 1)], np.int32)
    order = ((y + chip) % 4) * 2 + (core ^ side)
    dz = np.array([s[0] for s in sources()], np.int32)
    dx = np.array([s[1] for s in sources()], np.int32)
    earlier = (((z - dz) % 4) * 4 + (x - dx) % 4 < ep).astype(jnp.int32)
    flags = jnp.concatenate([earlier, order])
    inside = (order[:, None] * local + jnp.arange(local, dtype=jnp.int32)[None, :]).reshape(-1)
    place, freq = angles(ep * group + inside)
    angle = freq[:, None] * place[None, :]
    query_w = jnp.concatenate([query_nope_w, query_rope_w], axis=1).T
    one1, two1, one2, two2, low, high = heads(
        latents, key_up_w, value_up_w.T, query_w, jnp.cos(angle), jnp.sin(angle)
    )

    def line(one, two, send):
        below, above, far = ring(one, two, send)
        return [one, two, *below, *above, *far]

    a1, b1 = join(line(one1, two1, send_z))
    a2, b2 = join(line(one2, two2, send_x))
    wide1 = ring(a1, b1, send_x)
    wide2 = ring(a2, b2, send_z)
    state = own_attention(low, high, (one1, two1, one2, two2), inside, outputs)
    state = more_attention(low, high, (a1, b1, a2, b2), flags, 0, state)
    near = (*wide1[0], *wide1[1], *wide2[0], *wide2[1])
    state = more_attention(low, high, near, flags, 8, state)
    attended = more_attention(low, high, (*wide1[2], *wide2[2]), flags, 24, state, final=True)
    attended = lax.all_to_all(attended, "tp", split_axis=0, concat_axis=0, tiled=True)
    return project(attended, outputs, flags)


def per_device(
    query_latent,
    kv_latent,
    rope_key,
    query_gain,
    kv_gain,
    query_nope_w,
    query_rope_w,
    key_up_w,
    value_up_w,
    output_w,
    expert_in,
    moe_gain,
    routes,
    route_weight,
    gate_w,
    up_w,
    down_w,
):
    block = own_block(query_latent, kv_latent, rope_key, query_gain, kv_gain)
    mixer_out = mixer(
        query_latent,
        kv_latent,
        rope_key,
        query_gain,
        kv_gain,
        query_nope_w,
        query_rope_w,
        key_up_w,
        value_up_w,
        output_w,
        block,
    )
    expert_out = experts_half(
        expert_in, moe_gain, routes, route_weight, gate_w, up_w, down_w, block
    )
    return (mixer_out, expert_out)


def solution(mesh):
    placed = (
        P(("ep", "tp"), None),
        P(("ep", "tp"), None),
        P(("ep", "tp"), None),
        P(),
        P(),
        P(None, "tp"),
        P(None, "tp"),
        P(None, "tp"),
        P(None, "tp"),
        P("tp", None),
        P(("ep", "tp"), None),
        P(),
        P(("ep", "tp"), None),
        P(("ep", "tp"), None),
        P("ep", None, "tp"),
        P("ep", None, "tp"),
        P("ep", "tp", None),
    )
    return jax.shard_map(
        per_device,
        mesh=mesh,
        in_specs=placed,
        out_specs=(P(("ep", "tp"), None), P(("ep", "tp"), None)),
        check_vma=False,
    )
```

```python
import functools
import math

import jax
import jax.numpy as jnp
import numpy as np
from jax import lax
from jax.experimental import pallas as pl
from jax.experimental.pallas import tpu as pltpu
from jax.sharding import PartitionSpec as P


NOPE = 128
ROPE = 64
VDIM = 128
THETA = 10000.0
CHUNK = 24
HALF = 12
CAP = 10
BF = jnp.bfloat16
F32 = jnp.float32
LOG2E = 1.4426950408889634


def dot(a, b, dims=(((1,), (0,)), ((), ()))):
    return lax.dot_general(a, b, dims, preferred_element_type=F32)


def pairs(move):
    result = []
    for device in range(128):
        ep, tp = divmod(device, 8)
        z, x, y, core = ep // 4, ep % 4, tp // 2, tp % 2
        dz, dx, dy, dc = move(core)
        ep = ((z + dz) % 4) * 4 + (x + dx) % 4
        tp = ((y + dy) % 4) * 2 + (core ^ dc)
        result.append((device, ep * 8 + tp))
    return result


def send(a, move):
    return lax.ppermute(a, ("ep", "tp"), pairs(move))


def swap(a):
    return send(a, lambda core: (0, 0, 0, 1))


def along_y(d):
    return lambda core: (0, 0, -d if core else d, 0)


def plain_y(d):
    return lambda core: (0, 0, d, 0)


def along_one(d):
    return lambda core: (0, d, 0, 0) if core else (d, 0, 0, 0)


def along_two(d):
    return lambda core: (d, 0, 0, 0) if core else (0, d, 0, 0)


def ring(block, along):
    behind = send(block, along(1))
    ahead = send(block, along(-1))
    far = send(behind, along(1))
    return behind, ahead, far


def ring_halves(one, two, along):
    one_behind = send(one, along(1))
    two_ahead = send(two, along(-1))
    two_behind = send(two, along(1))
    one_ahead = send(one, along(-1))
    one_far = send(one_behind, along(1))
    two_far = send(two_ahead, along(-1))
    return (one_behind, two_behind), (one_ahead, two_ahead), (one_far, two_far)


def slots_of(route, rank):
    return (route >> 1) * CHUNK + (route & 1) * HALF + rank


def upright(row):
    count = row.shape[1]
    i = lax.broadcasted_iota(jnp.int32, (count, count), 0)
    j = lax.broadcasted_iota(jnp.int32, (count, count), 1)
    spread = jnp.where(i == j, row.astype(F32), 0.0)
    return jnp.sum(spread, axis=1, keepdims=True).astype(jnp.int32)


def dispatch_body(x_ref, gain_ref, row_ref, out_ref):
    floats = x_ref[...].astype(F32)
    center = floats - jnp.mean(floats, axis=-1, keepdims=True)
    variance = jnp.mean(center * center, axis=-1, keepdims=True)
    normed = (center * lax.rsqrt(variance + 1e-05) * gain_ref[...][None, :]).astype(BF)
    count = x_ref.shape[0]
    cols = [upright(row_ref[k : k + 1, :]) for k in range(2)]
    j = lax.broadcasted_iota(jnp.int32, (count, count), 0)
    i = lax.broadcasted_iota(jnp.int32, (count, count), 1)
    earlier = j < i
    total = out_ref.shape[0]
    number = lax.broadcasted_iota(jnp.int32, (total, count), 0)
    select = None
    for k in range(2):
        mine = row_ref[k : k + 1, :]
        same = (cols[0] == mine) | (cols[1] == mine)
        rank = jnp.sum(jnp.where(same & earlier, 1.0, 0.0), axis=0, keepdims=True)
        hit = number == slots_of(mine, rank.astype(jnp.int32))
        select = hit if select is None else select | hit
    pick = jnp.where(select, 1.0, 0.0).astype(BF)
    out_ref[...] = dot(pick, normed).astype(BF)


def dispatch(x, gain, routes):
    return pl.pallas_call(
        dispatch_body,
        out_shape=jax.ShapeDtypeStruct((16 * CHUNK, x.shape[1]), BF),
        name="dispatch",
    )(x, gain, routes.T)


def combine_body(back_ref, row_ref, w_ref, out_ref):
    count = row_ref.shape[1]
    i = lax.broadcasted_iota(jnp.int32, (count, count), 0)
    j = lax.broadcasted_iota(jnp.int32, (count, count), 1)
    earlier = j < i
    total = back_ref.shape[0]
    number = lax.broadcasted_iota(jnp.int32, (count, total), 1)
    weight = w_ref[...]
    weight = weight / jnp.sum(weight, axis=-1, keepdims=True)
    back = back_ref[...]
    result = None
    for k in range(2):
        mine = upright(row_ref[k : k + 1, :])
        same = (row_ref[0:1, :] == mine) | (row_ref[1:2, :] == mine)
        rank = jnp.sum(jnp.where(same & earlier, 1.0, 0.0), axis=1, keepdims=True)
        hit = number == slots_of(mine, rank.astype(jnp.int32))
        pick = jnp.where(hit, 1.0, 0.0).astype(BF)
        term = dot(pick, back) * weight[:, k : k + 1]
        result = term if result is None else result + term
    out_ref[...] = result.astype(BF)


def combine(back, routes, route_weight):
    return pl.pallas_call(
        combine_body,
        out_shape=jax.ShapeDtypeStruct((routes.shape[0], back.shape[1]), BF),
        name="combine",
    )(back, routes.T, route_weight)


def packing(flip):
    rows, cols = 16 * 2 * CAP, 16 * CHUNK
    shape = (cols, rows) if flip else (rows, cols)
    r = lax.broadcasted_iota(jnp.int32, shape, flip)
    c = lax.broadcasted_iota(jnp.int32, shape, 1 - flip)
    per = 16 * CAP
    slot = ((r % per) // CAP) * CHUNK + (r // per) * HALF + r % CAP
    return (slot == c).astype(BF)


def pack_body(pick_ref, x_ref, one_ref, two_ref):
    rows = one_ref.shape[0]
    packed = dot(pick_ref[...], x_ref[...]).astype(BF)
    one_ref[...] = packed[:rows]
    two_ref[...] = packed[rows:]


def columns(rows, width=512):
    return pl.BlockSpec((rows, width), lambda n: (0, n))


def whole(shape):
    return pl.BlockSpec(shape, lambda n: (0,) * len(shape))


def pack(pick, arrived):
    rows, width = arrived.shape
    half = pick.shape[0] // 2
    return pl.pallas_call(
        pack_body,
        grid=(2,),
        in_specs=[whole(pick.shape), columns(rows, width // 2)],
        out_specs=[columns(half, width // 2)] * 2,
        out_shape=[jax.ShapeDtypeStruct((half, width), BF)] * 2,
        name="pack",
    )(pick, arrived)


def unpack_body(pick_ref, *refs):
    out_ref = refs[-1]
    halves = []
    for k in range(2):
        a, b, c = refs[k:6:2]
        halves.append((a[...].astype(F32) + b[...].astype(F32) + c[...].astype(F32)).astype(BF))
    summed = jnp.concatenate(halves, axis=0)
    out_ref[...] = dot(pick_ref[...], summed).astype(BF)


def unpack(pick, *terms):
    rows, width = terms[0][0].shape
    return pl.pallas_call(
        unpack_body,
        grid=(2,),
        in_specs=[whole(pick.shape)] + [columns(rows, width // 2)] * 6,
        out_specs=columns(pick.shape[0], width // 2),
        out_shape=jax.ShapeDtypeStruct((pick.shape[0], width), BF),
        name="unpack",
    )(pick, *[a for pair in terms for a in pair])


def add_body(*refs):
    count = len(refs) // 3
    for k in range(count):
        a, b = refs[2 * k], refs[2 * k + 1]
        refs[2 * count + k][...] = (a[...].astype(F32) + b[...].astype(F32)).astype(BF)


def add(*pairs):
    rows, width = pairs[0][0].shape
    count = len(pairs)
    block = pl.BlockSpec((rows // 2, width), lambda n: (n, 0))
    return pl.pallas_call(
        add_body,
        grid=(2,),
        in_specs=[block] * 2 * count,
        out_specs=[block] * count,
        out_shape=[jax.ShapeDtypeStruct((rows, width), BF)] * count,
        name="add",
    )(*[a for pair in pairs for a in pair])


def ffn_body(count, *refs):
    xs = refs[: 2 * count]
    sources = refs[2 * count : 2 * count + 6]
    outs = refs[2 * count + 6 : 4 * count + 6]
    gates, uppers, downs, sems = refs[4 * count + 6 :]
    copies = []
    for expert in range(2):
        for half in range(2):
            for k, target in enumerate((gates, uppers, downs)):
                number = len(copies)
                copies.append(
                    pltpu.make_async_copy(
                        sources[half * 3 + k].at[expert],
                        target.at[expert * 2 + half],
                        sems.at[number],
                    )
                )
    for copy in copies:
        copy.start()
    rows = xs[0].shape[0]
    for expert in range(2):
        mine = xs[expert::2]
        x = mine[0][...] if count == 1 else jnp.concatenate([r[...] for r in mine], axis=0)
        hidden = []
        for half in range(2):
            at = expert * 2 + half
            for k in range(3):
                copies[at * 3 + k].wait()
            gate = jnp.minimum(dot(x, gates[at]), 7.0)
            upper = jnp.clip(dot(x, uppers[at]), -7.0, 7.0)
            hidden.append((gate * jax.nn.sigmoid(1.702 * gate) * (upper + 1.0)).astype(BF))
        total = dot(hidden[0], downs[expert * 2]) + dot(hidden[1], downs[expert * 2 + 1])
        total = total.astype(BF)
        for k in range(count):
            outs[2 * k + expert][...] = total[k * rows : (k + 1) * rows]


def ffn(weights, *xs):
    rows, width = xs[0][0].shape
    count = len(xs)
    inner = weights[0].shape[2]
    vmem = pl.BlockSpec(memory_space=pltpu.VMEM)
    out = jax.ShapeDtypeStruct((rows, width), BF)
    outs = pl.pallas_call(
        functools.partial(ffn_body, count),
        in_specs=[vmem] * 2 * count + [pl.BlockSpec(memory_space=pl.ANY)] * 6,
        out_specs=[vmem] * 2 * count,
        out_shape=[out] * 2 * count,
        scratch_shapes=[
            pltpu.VMEM((4, width, inner), BF),
            pltpu.VMEM((4, width, inner), BF),
            pltpu.VMEM((4, inner, width), BF),
            pltpu.SemaphoreType.DMA((12,)),
        ],
        cost_estimate=pl.CostEstimate(
            flops=12 * rows * count * width * 512, bytes_accessed=16 << 20, transcendentals=0
        ),
        name="ffn",
    )(*[a for pair in xs for a in pair], *weights)
    return [tuple(outs[2 * k : 2 * k + 2]) for k in range(count)]


def experts_half(
    expert_in, moe_gain, routes, route_weight, gate_w, up_w, down_w
):
    width = expert_in.shape[1]
    outgoing = dispatch(expert_in, moe_gain, routes)
    weights = (gate_w, up_w, down_w, swap(gate_w), swap(up_w), swap(down_w))
    arrived = lax.all_to_all(
        outgoing.reshape(16, CHUNK, width), "ep", split_axis=0, concat_axis=0, tiled=True
    ).reshape(16 * CHUNK, width)
    own = pack(packing(0), arrived)
    below, above, far = ring_halves(*own, plain_y)
    (below0, above1), own_out = ffn(weights, (below[0], above[1]), own)
    from_above0 = send(below0, plain_y(-1))
    from_below1 = send(above1, plain_y(1))
    (far0, far1), (above0, below1) = ffn(weights, far, (above[0], below[1]))
    far0 = send(far0, plain_y(1))
    far1 = send(far1, plain_y(-1))
    above0, below1 = add((above0, far0), (below1, far1))
    from_below0 = send(above0, plain_y(1))
    from_above1 = send(below1, plain_y(-1))
    back = unpack(packing(1), own_out, (from_below0, from_below1), (from_above0, from_above1))
    back = lax.all_to_all(
        back.reshape(16, CHUNK, width), "ep", split_axis=0, concat_axis=0, tiled=True
    ).reshape(16 * CHUNK, width)
    return combine(back, routes, route_weight)


SCALE2 = LOG2E / math.sqrt(NOPE + ROPE)
QLAT = 768
KVLAT = 512
LATENT = 1536
KEYS = 512
PIECE = KEYS + KEYS // 2 + 4 * VDIM
NT = (((1,), (1,)), ((), ()))
LIMIT = 2.0**80


def prepare_body(q_ref, kv_ref, rot_ref, qg_ref, kvg_ref, out_ref):
    for ref, gain, at in ((q_ref, qg_ref, 0), (kv_ref, kvg_ref, QLAT)):
        floats = ref[...].astype(F32)
        square = jnp.mean(floats * floats, axis=-1, keepdims=True)
        normed = floats * lax.rsqrt(square + 1e-06) * gain[...][None, :]
        out_ref[:, at : at + ref.shape[1]] = normed.astype(BF)
    rot = rot_ref[...]
    both = jnp.concatenate([rot, jnp.zeros_like(rot)], axis=1)
    out_ref[:, QLAT + KVLAT : QLAT + KVLAT + 128] = both
    out_ref[:, QLAT + KVLAT + 128 :] = jnp.zeros((rot.shape[0], 128), BF)


def prepare(query_latent, kv_latent, key_rot, query_gain, kv_gain):
    return pl.pallas_call(
        prepare_body,
        out_shape=jax.ShapeDtypeStruct((query_latent.shape[0], LATENT), BF),
        name="prepare",
    )(query_latent, kv_latent, key_rot, query_gain, kv_gain)


def heads_body(*refs):
    blocks = refs[:8]
    key_ref, value_ref, nope_ref, rope_ref, cos_ref, sin_ref = refs[8:14]
    kv_ref, low_ref, high_ref = refs[14:]
    kv = jnp.concatenate([r[:, QLAT : QLAT + KVLAT] for r in blocks], axis=0)
    keys = dot(kv, key_ref[...]).astype(BF)
    values = dot(value_ref[...].T, kv, NT).astype(BF)
    rots = jnp.concatenate(
        [r[:, QLAT + KVLAT : QLAT + KVLAT + 128] for r in blocks], axis=0
    ).astype(F32)
    half = KEYS // 2
    for k in range(2):
        at = k * KEYS
        to = k * PIECE
        pair = rots[at : at + half] + pltpu.roll(rots[at + half : at + KEYS], ROPE, 1)
        kv_ref[to : to + KEYS, :] = keys[at : at + KEYS]
        kv_ref[to + KEYS : to + KEYS + half, :] = pair.astype(BF)
        for c in range(4):
            row = to + KEYS + half + 128 * c
            kv_ref[row : row + 128, :] = values[:, at + 128 * c : at + 128 * (c + 1)]
    query_in = jnp.concatenate([r[:, :QLAT] for r in blocks], axis=0)
    query = dot(jnp.concatenate([nope_ref[...].T, rope_ref[...]], axis=0), query_in, NT)
    first = query[NOPE : NOPE + ROPE // 2]
    second = query[NOPE + ROPE // 2 :]
    cosine = cos_ref[...]
    sine = sin_ref[...]
    rot = jnp.concatenate([first * cosine - second * sine, second * cosine + first * sine], axis=0)
    nope = query[:NOPE].astype(BF)
    rot = rot.astype(BF)
    blank = jnp.zeros_like(rot)
    low_ref[...] = jnp.concatenate([nope, rot, blank], axis=0)
    high_ref[...] = jnp.concatenate([nope, blank, rot], axis=0)


def heads(blocks, key_w, value_w, nope_w, rope_w, cosine, sine):
    rows = 8 * blocks[0].shape[0]
    query = jax.ShapeDtypeStruct((256, rows), BF)
    return pl.pallas_call(
        heads_body,
        out_shape=[jax.ShapeDtypeStruct((2 * PIECE, 128), BF), query, query],
        cost_estimate=pl.CostEstimate(
            flops=2 * rows * (QLAT * 192 + KVLAT * 256), bytes_accessed=6 << 20, transcendentals=0
        ),
        name="heads",
    )(*blocks, key_w, value_w, nope_w, rope_w.T, cosine, sine)


def join_body(a_ref, b_ref, c_ref, d_ref, one_ref, two_ref):
    rows = a_ref.shape[0]
    one_ref[:rows, :] = a_ref[...]
    one_ref[rows:, :] = b_ref[...]
    two_ref[:rows, :] = c_ref[...]
    two_ref[rows:, :] = d_ref[...]


def join(blocks):
    rows = blocks[0].shape[0]
    out = jax.ShapeDtypeStruct((2 * rows, 128), BF)
    return pl.pallas_call(join_body, out_shape=[out] * 2, name="join")(*blocks)


def load_piece(ref, k):
    at = pl.multiple_of(k * PIECE, PIECE)
    half = KEYS // 2
    pair = ref[pl.ds(at + KEYS, half), :]
    left = jnp.concatenate([ref[pl.ds(at, half), :], pair], axis=1)
    right = jnp.concatenate([ref[pl.ds(at + half, half), :], pair], axis=1)
    value = [ref[pl.ds(at + KEYS + half + 128 * c, 128), :] for c in range(4)]
    return left, right, jnp.concatenate(value, axis=1)


def own_body(kpos_ref, qpos_ref, low_ref, high_ref, kv_ref, *refs):
    m_ref, l_ref, acc_ref = refs[-3:]
    tile = 256
    half = KEYS // 2
    pieces = [load_piece(kv_ref, k) for k in range(2)]
    lefts = [pieces[0][0], pieces[0][1], pieces[1][0], pieces[1][1]]
    value = jnp.concatenate([pieces[0][2], pieces[1][2]], axis=1)
    for part in range(low_ref.shape[1] // tile):
        cols = slice(part * tile, (part + 1) * tile)
        scores = []
        for k, left in enumerate(lefts):
            s = dot(left, (high_ref if k % 2 else low_ref)[:, cols])
            allowed = kpos_ref[k * half : (k + 1) * half, :] <= qpos_ref[:, cols]
            scores.append(jnp.where(allowed, s, -1e30))
        peaks = [jnp.max(s, axis=0, keepdims=True) for s in scores]
        m = jnp.maximum(jnp.maximum(peaks[0], peaks[1]), jnp.maximum(peaks[2], peaks[3]))
        base = m * SCALE2
        probs = [jnp.exp2(s * SCALE2 - base) for s in scores]
        sums = [jnp.sum(p, axis=0, keepdims=True) for p in probs]
        m_ref[:, cols] = m
        l_ref[:, cols] = (sums[0] + sums[1]) + (sums[2] + sums[3])
        acc_ref[:, cols] = dot(value, jnp.concatenate([p.astype(BF) for p in probs], axis=0))


def own_attention(low, high, kv, positions):
    rows = low.shape[1]
    thin = jax.ShapeDtypeStruct((1, rows), F32)
    vmem = pl.BlockSpec(memory_space=pltpu.VMEM)
    return pl.pallas_call(
        own_body,
        in_specs=[vmem] * 5,
        out_specs=[vmem] * 3,
        out_shape=[thin, thin, jax.ShapeDtypeStruct((VDIM, rows), F32)],
        cost_estimate=pl.CostEstimate(
            flops=2 * rows * rows * 384, bytes_accessed=4 << 20, transcendentals=rows * rows
        ),
        name="own_attention",
    )(positions.reshape(-1, 1), positions.reshape(1, -1), low, high, kv)


def more_body(arrays, first, final, flags_ref, low_ref, high_ref, *refs):
    pieces = refs[:arrays]
    m_in, l_in, acc_in = refs[arrays : arrays + 3]
    if final:
        m_ref, l_ref, acc_ref = refs[arrays + 7 :]
    else:
        m_ref, l_ref, acc_ref = refs[arrays + 3 :]
    tile = 256
    tiles = low_ref.shape[1] // tile

    def start():
        m_ref[...] = m_in[...]
        l_ref[...] = l_in[...]
        acc_ref[...] = acc_in[...]

    def score(piece, t):
        cols = slice(t * tile, (t + 1) * tile)
        return dot(piece[0], low_ref[:, cols]), dot(piece[1], high_ref[:, cols])

    def over(step):
        for number, ref in enumerate(pieces):

            def one(k, _, ref=ref, number=number):
                @pl.when(flags_ref[first + 2 * number + k] != 0)
                def _():
                    step(ref, k)

                return 0

            lax.fori_loop(0, 2, one, 0)

    def weigh(s, t):
        cols = slice(t * tile, (t + 1) * tile)
        base = m_ref[:, cols] * SCALE2
        p = jnp.exp2(s[0] * SCALE2 - base)
        q = jnp.exp2(s[1] * SCALE2 - base)
        l_ref[:, cols] += jnp.sum(p, axis=0, keepdims=True) + jnp.sum(q, axis=0, keepdims=True)
        return jnp.concatenate([p.astype(BF), q.astype(BF)], axis=0)

    def gather(piece, probs, t):
        cols = slice(t * tile, (t + 1) * tile)
        acc_ref[:, cols] += dot(piece[2], probs)

    def quick(ref, k):
        block = [load_piece(ref, 2 * k), load_piece(ref, 2 * k + 1)]
        steps = [(piece, t) for piece in block for t in range(tiles)]
        s = score(*steps[0])
        before = None
        for i, (_, t) in enumerate(steps):
            after = score(*steps[i + 1]) if i + 1 < len(steps) else None
            if before is not None:
                gather(steps[i - 1][0], before, steps[i - 1][1])
            before = weigh(s, t)
            s = after
        gather(steps[-1][0], before, steps[-1][1])

    def careful(ref, k):
        def one(i, _):
            piece = load_piece(ref, 2 * k + i // tiles)
            cols = pl.ds(pl.multiple_of((i % tiles) * tile, tile), tile)
            p = dot(piece[0], low_ref[:, cols])
            q = dot(piece[1], high_ref[:, cols])
            before = m_ref[:, cols]
            peak = jnp.maximum(jnp.max(p, axis=0, keepdims=True), jnp.max(q, axis=0, keepdims=True))
            m = jnp.maximum(before, peak)
            alpha = jnp.exp2((before - m) * SCALE2)
            p = jnp.exp2(p * SCALE2 - m * SCALE2)
            q = jnp.exp2(q * SCALE2 - m * SCALE2)
            m_ref[:, cols] = m
            total = jnp.sum(p, axis=0, keepdims=True) + jnp.sum(q, axis=0, keepdims=True)
            l_ref[:, cols] = l_ref[:, cols] * alpha + total
            probs = jnp.concatenate([p.astype(BF), q.astype(BF)], axis=0)
            acc_ref[:, cols] = acc_ref[:, cols] * alpha + dot(piece[2], probs)
            return 0

        lax.fori_loop(0, 2 * tiles, one, 0)

    start()
    over(quick)
    safe = jnp.where(l_ref[...] < LIMIT, 0.0, 1.0)

    @pl.when(jnp.max(safe) > 0.0)
    def _():
        start()
        over(careful)

    if final:
        done = (acc_ref[...] / l_ref[...]).astype(BF)
        for b in range(4):
            refs[arrays + 3 + b][...] = done[:, 256 * b : 256 * (b + 1)]


def more_attention(low, high, arrays, flags, first, state, final=False):
    rows = low.shape[1]
    keys = 4 * len(arrays) * KEYS
    shapes = [(1, rows), (1, rows), (VDIM, rows)]
    if final:
        out_shape = [jax.ShapeDtypeStruct((VDIM, rows // 4), BF)] * 4
        scratch = [pltpu.VMEM(s, F32) for s in shapes]
    else:
        out_shape = [jax.ShapeDtypeStruct(s, F32) for s in shapes]
        scratch = []
    vmem = pl.BlockSpec(memory_space=pltpu.VMEM)
    return pl.pallas_call(
        functools.partial(more_body, len(arrays), first, final),
        in_specs=[pl.BlockSpec(memory_space=pltpu.SMEM)] + [vmem] * (5 + len(arrays)),
        out_specs=[vmem] * len(out_shape),
        out_shape=out_shape,
        scratch_shapes=scratch,
        cost_estimate=pl.CostEstimate(
            flops=rows * keys * 384, bytes_accessed=4 << 20, transcendentals=rows * keys
        ),
        name="more_attention",
    )(flags, low, high, *arrays, *state)


def project_body(*refs):
    left = jnp.concatenate([r[...] for r in refs[:4]], axis=0)
    right = jnp.concatenate([r[...] for r in refs[4:8]], axis=0)
    mine, other = refs[8:]
    result = dot(left, right, (((0,), (0,)), ((), ())))
    rows = mine.shape[0]
    mine[...] = result[:rows]
    other[...] = result[rows:].astype(BF)


def project(attended, blocks):
    rows = attended[0].shape[1] // 2
    width = blocks[0].shape[1]
    return pl.pallas_call(
        project_body,
        grid=(width // 512,),
        in_specs=[whole(a.shape) for a in attended] + [columns(128)] * 4,
        out_specs=[columns(rows)] * 2,
        out_shape=[
            jax.ShapeDtypeStruct((rows, width), F32),
            jax.ShapeDtypeStruct((rows, width), BF),
        ],
        name="project",
    )(*attended, *blocks)


def angles(positions):
    half = ROPE // 2
    freq = 1.0 / THETA ** (jnp.arange(half, dtype=F32) * 2.0 / ROPE)
    return positions.astype(F32), freq


def turn(values):
    half = ROPE // 2
    return jnp.concatenate([-values[:, half:], values[:, :half]], axis=-1)


LINE = (0, 1, -1, 2)


def sources():
    near = [(d, 0) for d in LINE]
    wide = [(a, b) for b in (1, -1) for a in LINE]
    far = [(a, 2) for a in LINE]
    return near + wide + far


def own_block(query_latent, kv_latent, rope_key, query_gain, kv_gain):
    local = query_latent.shape[0]
    first = (lax.axis_index("ep") * 8 + lax.axis_index("tp")) * local
    place, freq = angles(first + jnp.arange(local, dtype=jnp.int32))
    angle = place[:, None] * freq[None, :]
    angle = jnp.concatenate([angle, angle], axis=-1)
    key_in = rope_key.astype(F32)
    key_rot = (key_in * jnp.cos(angle) + turn(key_in) * jnp.sin(angle)).astype(BF)
    return prepare(query_latent, kv_latent, key_rot, query_gain, kv_gain)


def mixer(query_latent, query_nope_w, query_rope_w, key_up_w, value_up_w, output_w, block):
    local = query_latent.shape[0]
    group = local * 8
    ep = lax.axis_index("ep")
    tp = lax.axis_index("tp")
    z, x = ep // 4, ep % 4
    y, core = tp // 2, tp % 2
    behind, ahead, far = ring(block, along_y)
    outputs = (output_w, *ring(output_w, along_y))
    blocks = [block, swap(block), behind, swap(ahead), ahead, swap(behind), far, swap(far)]
    turned = 1 - 2 * core
    chips = (y + turned * np.array([0, -1, 1, 2], np.int32)) % 4
    one = np.array([s[0] for s in sources()], np.int32)
    two = np.array([s[1] for s in sources()], np.int32)
    dz = jnp.where(core == 0, one, two)
    dx = jnp.where(core == 0, two, one)
    flags = (((z - dz) % 4) * 4 + (x - dx) % 4 < ep).astype(jnp.int32)
    order = chips[:, None] * 2 + (core ^ np.array([[0, 1]], np.int32))
    inside = (order.reshape(8, 1) * local + np.arange(local, dtype=np.int32)[None, :]).reshape(-1)
    place, freq = angles(ep * group + inside)
    angle = freq[:, None] * place[None, :]
    turns = jnp.cos(angle), jnp.sin(angle)
    kv, low, high = heads(blocks, key_up_w, value_up_w, query_nope_w, query_rope_w, *turns)
    one, two = join([kv, *ring(kv, along_one)])
    behind, ahead, far = ring_halves(one, two, along_two)
    state = own_attention(low, high, kv, inside)
    state = more_attention(low, high, (one, two), flags, 0, state)
    state = more_attention(low, high, (*behind, *ahead), flags, 4, state)
    attended = more_attention(low, high, far, flags, 12, state, final=True)
    attended = (
        attended[0],
        send(attended[2], along_y(1)),
        send(attended[1], along_y(-1)),
        send(attended[3], along_y(2)),
    )
    mine, other = project(attended, outputs)
    return add((mine, swap(other)))[0]


def per_device(
    query_latent,
    kv_latent,
    rope_key,
    query_gain,
    kv_gain,
    query_nope_w,
    query_rope_w,
    key_up_w,
    value_up_w,
    output_w,
    expert_in,
    moe_gain,
    routes,
    route_weight,
    gate_w,
    up_w,
    down_w,
):
    block = own_block(query_latent, kv_latent, rope_key, query_gain, kv_gain)
    mixer_out = mixer(
        query_latent, query_nope_w, query_rope_w, key_up_w, value_up_w, output_w, block
    )
    expert_out = experts_half(
        expert_in, moe_gain, routes, route_weight, gate_w, up_w, down_w
    )
    return (mixer_out, expert_out)


def solution(mesh):
    placed = (
        P(("ep", "tp"), None),
        P(("ep", "tp"), None),
        P(("ep", "tp"), None),
        P(),
        P(),
        P(None, "tp"),
        P(None, "tp"),
        P(None, "tp"),
        P(None, "tp"),
        P("tp", None),
        P(("ep", "tp"), None),
        P(),
        P(("ep", "tp"), None),
        P(("ep", "tp"), None),
        P("ep", None, "tp"),
        P("ep", None, "tp"),
        P("ep", "tp", None),
    )
    return jax.shard_map(
        per_device,
        mesh=mesh,
        in_specs=placed,
        out_specs=(P(("ep", "tp"), None), P(("ep", "tp"), None)),
        check_vma=False,
    )
```

```python
import functools
import math

import jax
import jax.numpy as jnp
import numpy as np
from jax import lax
from jax.experimental import pallas as pl
from jax.experimental.pallas import tpu as pltpu
from jax.sharding import PartitionSpec as P


NOPE = 128
ROPE = 64
VDIM = 128
THETA = 10000.0
CHUNK = 24
HALF = 12
CAP = 10
BF = jnp.bfloat16
F32 = jnp.float32
LOG2E = 1.4426950408889634


def dot(a, b, dims=(((1,), (0,)), ((), ()))):
    return lax.dot_general(a, b, dims, preferred_element_type=F32)


def pairs(move):
    result = []
    for device in range(128):
        ep, tp = divmod(device, 8)
        z, x, y, core = ep // 4, ep % 4, tp // 2, tp % 2
        dz, dx, dy, dc = move(core)
        ep = ((z + dz) % 4) * 4 + (x + dx) % 4
        tp = ((y + dy) % 4) * 2 + (core ^ dc)
        result.append((device, ep * 8 + tp))
    return result


def send(a, move):
    return lax.ppermute(a, ("ep", "tp"), pairs(move))


def swap(a):
    return send(a, lambda core: (0, 0, 0, 1))


def along_y(d):
    return lambda core: (0, 0, -d if core else d, 0)


def plain_y(d):
    return lambda core: (0, 0, d, 0)


def along_one(d):
    return lambda core: (0, d, 0, 0) if core else (d, 0, 0, 0)


def along_two(d):
    return lambda core: (d, 0, 0, 0) if core else (0, d, 0, 0)


def ring(block, along):
    behind = send(block, along(1))
    ahead = send(block, along(-1))
    far = send(behind, along(1))
    return behind, ahead, far


def ring_halves(one, two, along):
    one_behind = send(one, along(1))
    two_ahead = send(two, along(-1))
    two_behind = send(two, along(1))
    one_ahead = send(one, along(-1))
    one_far = send(one_behind, along(1))
    two_far = send(two_ahead, along(-1))
    return (one_behind, two_behind), (one_ahead, two_ahead), (one_far, two_far)


def slots_of(route, rank):
    return (route >> 1) * CHUNK + (route & 1) * HALF + rank


def upright(row):
    count = row.shape[1]
    i = lax.broadcasted_iota(jnp.int32, (count, count), 0)
    j = lax.broadcasted_iota(jnp.int32, (count, count), 1)
    spread = jnp.where(i == j, row.astype(F32), 0.0)
    return jnp.sum(spread, axis=1, keepdims=True).astype(jnp.int32)


def dispatch_body(x_ref, gain_ref, row_ref, out_ref):
    floats = x_ref[...].astype(F32)
    center = floats - jnp.mean(floats, axis=-1, keepdims=True)
    variance = jnp.mean(center * center, axis=-1, keepdims=True)
    normed = (center * lax.rsqrt(variance + 1e-05) * gain_ref[...][None, :]).astype(BF)
    count = x_ref.shape[0]
    cols = [upright(row_ref[k : k + 1, :]) for k in range(2)]
    j = lax.broadcasted_iota(jnp.int32, (count, count), 0)
    i = lax.broadcasted_iota(jnp.int32, (count, count), 1)
    earlier = j < i
    total = out_ref.shape[0]
    number = lax.broadcasted_iota(jnp.int32, (total, count), 0)
    select = None
    for k in range(2):
        mine = row_ref[k : k + 1, :]
        same = (cols[0] == mine) | (cols[1] == mine)
        rank = jnp.sum(jnp.where(same & earlier, 1.0, 0.0), axis=0, keepdims=True)
        hit = number == slots_of(mine, rank.astype(jnp.int32))
        select = hit if select is None else select | hit
    pick = jnp.where(select, 1.0, 0.0).astype(BF)
    out_ref[...] = dot(pick, normed).astype(BF)


def dispatch(x, gain, routes):
    return pl.pallas_call(
        dispatch_body,
        out_shape=jax.ShapeDtypeStruct((16 * CHUNK, x.shape[1]), BF),
        name="dispatch",
    )(x, gain, routes.T)


def combine_body(back_ref, row_ref, w_ref, out_ref):
    count = row_ref.shape[1]
    i = lax.broadcasted_iota(jnp.int32, (count, count), 0)
    j = lax.broadcasted_iota(jnp.int32, (count, count), 1)
    earlier = j < i
    total = back_ref.shape[0]
    number = lax.broadcasted_iota(jnp.int32, (count, total), 1)
    weight = w_ref[...]
    weight = weight / jnp.sum(weight, axis=-1, keepdims=True)
    back = back_ref[...]
    result = None
    for k in range(2):
        mine = upright(row_ref[k : k + 1, :])
        same = (row_ref[0:1, :] == mine) | (row_ref[1:2, :] == mine)
        rank = jnp.sum(jnp.where(same & earlier, 1.0, 0.0), axis=1, keepdims=True)
        hit = number == slots_of(mine, rank.astype(jnp.int32))
        pick = jnp.where(hit, 1.0, 0.0).astype(BF)
        term = dot(pick, back) * weight[:, k : k + 1]
        result = term if result is None else result + term
    out_ref[...] = result.astype(BF)


def combine(back, routes, route_weight):
    return pl.pallas_call(
        combine_body,
        out_shape=jax.ShapeDtypeStruct((routes.shape[0], back.shape[1]), BF),
        name="combine",
    )(back, routes.T, route_weight)


def packing(flip):
    rows, cols = 16 * 2 * CAP, 16 * CHUNK
    shape = (cols, rows) if flip else (rows, cols)
    r = lax.broadcasted_iota(jnp.int32, shape, flip)
    c = lax.broadcasted_iota(jnp.int32, shape, 1 - flip)
    per = 16 * CAP
    slot = ((r % per) // CAP) * CHUNK + (r // per) * HALF + r % CAP
    return (slot == c).astype(BF)


def pack_body(pick_ref, x_ref, one_ref, two_ref):
    rows = one_ref.shape[0]
    packed = dot(pick_ref[...], x_ref[...]).astype(BF)
    one_ref[...] = packed[:rows]
    two_ref[...] = packed[rows:]


def columns(rows, width=512):
    return pl.BlockSpec((rows, width), lambda n: (0, n))


def whole(shape):
    return pl.BlockSpec(shape, lambda n: (0,) * len(shape))


def pack(pick, arrived):
    rows, width = arrived.shape
    half = pick.shape[0] // 2
    return pl.pallas_call(
        pack_body,
        grid=(2,),
        in_specs=[whole(pick.shape), columns(rows, width // 2)],
        out_specs=[columns(half, width // 2)] * 2,
        out_shape=[jax.ShapeDtypeStruct((half, width), BF)] * 2,
        name="pack",
    )(pick, arrived)


def unpack_body(pick_ref, *refs):
    out_ref = refs[-1]
    halves = []
    for k in range(2):
        a, b, c = refs[k:6:2]
        halves.append((a[...].astype(F32) + b[...].astype(F32) + c[...].astype(F32)).astype(BF))
    summed = jnp.concatenate(halves, axis=0)
    out_ref[...] = dot(pick_ref[...], summed).astype(BF)


def unpack(pick, *terms):
    rows, width = terms[0][0].shape
    return pl.pallas_call(
        unpack_body,
        grid=(2,),
        in_specs=[whole(pick.shape)] + [columns(rows, width // 2)] * 6,
        out_specs=columns(pick.shape[0], width // 2),
        out_shape=jax.ShapeDtypeStruct((pick.shape[0], width), BF),
        name="unpack",
    )(pick, *[a for pair in terms for a in pair])


def add_body(*refs):
    count = len(refs) // 3
    for k in range(count):
        a, b = refs[2 * k], refs[2 * k + 1]
        refs[2 * count + k][...] = (a[...].astype(F32) + b[...].astype(F32)).astype(BF)


def add(*pairs):
    rows, width = pairs[0][0].shape
    count = len(pairs)
    block = pl.BlockSpec((rows // 2, width), lambda n: (n, 0))
    return pl.pallas_call(
        add_body,
        grid=(2,),
        in_specs=[block] * 2 * count,
        out_specs=[block] * count,
        out_shape=[jax.ShapeDtypeStruct((rows, width), BF)] * count,
        name="add",
    )(*[a for pair in pairs for a in pair])


def ffn_body(count, *refs):
    xs = refs[: 2 * count]
    sources = refs[2 * count : 2 * count + 6]
    outs = refs[2 * count + 6 : 4 * count + 6]
    gates, uppers, downs, sems = refs[4 * count + 6 :]
    copies = []
    for expert in range(2):
        for half in range(2):
            for k, target in enumerate((gates, uppers, downs)):
                number = len(copies)
                copies.append(
                    pltpu.make_async_copy(
                        sources[half * 3 + k].at[expert],
                        target.at[expert * 2 + half],
                        sems.at[number],
                    )
                )
    for copy in copies:
        copy.start()
    rows = xs[0].shape[0]
    for expert in range(2):
        mine = xs[expert::2]
        x = mine[0][...] if count == 1 else jnp.concatenate([r[...] for r in mine], axis=0)
        hidden = []
        for half in range(2):
            at = expert * 2 + half
            for k in range(3):
                copies[at * 3 + k].wait()
            gate = jnp.minimum(dot(x, gates[at]), 7.0)
            upper = jnp.clip(dot(x, uppers[at]), -7.0, 7.0)
            hidden.append((gate * jax.nn.sigmoid(1.702 * gate) * (upper + 1.0)).astype(BF))
        total = dot(hidden[0], downs[expert * 2]) + dot(hidden[1], downs[expert * 2 + 1])
        total = total.astype(BF)
        for k in range(count):
            outs[2 * k + expert][...] = total[k * rows : (k + 1) * rows]


def ffn(weights, *xs):
    rows, width = xs[0][0].shape
    count = len(xs)
    inner = weights[0].shape[2]
    vmem = pl.BlockSpec(memory_space=pltpu.VMEM)
    out = jax.ShapeDtypeStruct((rows, width), BF)
    outs = pl.pallas_call(
        functools.partial(ffn_body, count),
        in_specs=[vmem] * 2 * count + [pl.BlockSpec(memory_space=pl.ANY)] * 6,
        out_specs=[vmem] * 2 * count,
        out_shape=[out] * 2 * count,
        scratch_shapes=[
            pltpu.VMEM((4, width, inner), BF),
            pltpu.VMEM((4, width, inner), BF),
            pltpu.VMEM((4, inner, width), BF),
            pltpu.SemaphoreType.DMA((12,)),
        ],
        cost_estimate=pl.CostEstimate(
            flops=12 * rows * count * width * 512, bytes_accessed=16 << 20, transcendentals=0
        ),
        name="ffn",
    )(*[a for pair in xs for a in pair], *weights)
    return [tuple(outs[2 * k : 2 * k + 2]) for k in range(count)]


def experts_half(
    expert_in, moe_gain, routes, route_weight, gate_w, up_w, down_w
):
    width = expert_in.shape[1]
    outgoing = dispatch(expert_in, moe_gain, routes)
    weights = (gate_w, up_w, down_w, swap(gate_w), swap(up_w), swap(down_w))
    arrived = lax.all_to_all(
        outgoing.reshape(16, CHUNK, width), "ep", split_axis=0, concat_axis=0, tiled=True
    ).reshape(16 * CHUNK, width)
    own = pack(packing(0), arrived)
    below, above, far = ring_halves(*own, plain_y)
    (below0, above1), own_out = ffn(weights, (below[0], above[1]), own)
    from_above0 = send(below0, plain_y(-1))
    from_below1 = send(above1, plain_y(1))
    (far0, far1), (above0, below1) = ffn(weights, far, (above[0], below[1]))
    far0 = send(far0, plain_y(1))
    far1 = send(far1, plain_y(-1))
    above0, below1 = add((above0, far0), (below1, far1))
    from_below0 = send(above0, plain_y(1))
    from_above1 = send(below1, plain_y(-1))
    back = unpack(packing(1), own_out, (from_below0, from_below1), (from_above0, from_above1))
    back = lax.all_to_all(
        back.reshape(16, CHUNK, width), "ep", split_axis=0, concat_axis=0, tiled=True
    ).reshape(16 * CHUNK, width)
    return combine(back, routes, route_weight)


SCALE2 = LOG2E / math.sqrt(NOPE + ROPE)
QLAT = 768
KVLAT = 512
LATENT = 1536
KEYS = 512
PIECE = KEYS + KEYS // 2 + 4 * VDIM
NT = (((1,), (1,)), ((), ()))
LIMIT = 2.0**80


def prepare_body(q_ref, kv_ref, rot_ref, qg_ref, kvg_ref, out_ref):
    for ref, gain, at in ((q_ref, qg_ref, 0), (kv_ref, kvg_ref, QLAT)):
        floats = ref[...].astype(F32)
        square = jnp.mean(floats * floats, axis=-1, keepdims=True)
        normed = floats * lax.rsqrt(square + 1e-06) * gain[...][None, :]
        out_ref[:, at : at + ref.shape[1]] = normed.astype(BF)
    rot = rot_ref[...]
    both = jnp.concatenate([rot, jnp.zeros_like(rot)], axis=1)
    out_ref[:, QLAT + KVLAT : QLAT + KVLAT + 128] = both
    out_ref[:, QLAT + KVLAT + 128 :] = jnp.zeros((rot.shape[0], 128), BF)


def prepare(query_latent, kv_latent, key_rot, query_gain, kv_gain):
    return pl.pallas_call(
        prepare_body,
        out_shape=jax.ShapeDtypeStruct((query_latent.shape[0], LATENT), BF),
        name="prepare",
    )(query_latent, kv_latent, key_rot, query_gain, kv_gain)


def heads_body(*refs):
    blocks = refs[:8]
    key_ref, value_ref, nope_ref, rope_ref, cos_ref, sin_ref = refs[8:14]
    kv_ref, low_ref, high_ref = refs[14:]
    kv = jnp.concatenate([r[:, QLAT : QLAT + KVLAT] for r in blocks], axis=0)
    keys = dot(kv, key_ref[...]).astype(BF)
    values = dot(value_ref[...].T, kv, NT).astype(BF)
    rots = jnp.concatenate(
        [r[:, QLAT + KVLAT : QLAT + KVLAT + 128] for r in blocks], axis=0
    ).astype(F32)
    half = KEYS // 2
    for k in range(2):
        at = k * KEYS
        to = k * PIECE
        pair = rots[at : at + half] + pltpu.roll(rots[at + half : at + KEYS], ROPE, 1)
        kv_ref[to : to + KEYS, :] = keys[at : at + KEYS]
        kv_ref[to + KEYS : to + KEYS + half, :] = pair.astype(BF)
        for c in range(4):
            row = to + KEYS + half + 128 * c
            kv_ref[row : row + 128, :] = values[:, at + 128 * c : at + 128 * (c + 1)]
    query_in = jnp.concatenate([r[:, :QLAT] for r in blocks], axis=0)
    query = dot(jnp.concatenate([nope_ref[...].T, rope_ref[...]], axis=0), query_in, NT)
    first = query[NOPE : NOPE + ROPE // 2]
    second = query[NOPE + ROPE // 2 :]
    cosine = cos_ref[...]
    sine = sin_ref[...]
    rot = jnp.concatenate([first * cosine - second * sine, second * cosine + first * sine], axis=0)
    nope = query[:NOPE].astype(BF)
    rot = rot.astype(BF)
    blank = jnp.zeros_like(rot)
    low_ref[...] = jnp.concatenate([nope, rot, blank], axis=0)
    high_ref[...] = jnp.concatenate([nope, blank, rot], axis=0)


def heads(blocks, key_w, value_w, nope_w, rope_w, cosine, sine):
    rows = 8 * blocks[0].shape[0]
    query = jax.ShapeDtypeStruct((256, rows), BF)
    return pl.pallas_call(
        heads_body,
        out_shape=[jax.ShapeDtypeStruct((2 * PIECE, 128), BF), query, query],
        cost_estimate=pl.CostEstimate(
            flops=2 * rows * (QLAT * 192 + KVLAT * 256), bytes_accessed=6 << 20, transcendentals=0
        ),
        name="heads",
    )(*blocks, key_w, value_w, nope_w, rope_w.T, cosine, sine)


def join_body(a_ref, b_ref, c_ref, d_ref, one_ref, two_ref):
    rows = a_ref.shape[0]
    one_ref[:rows, :] = a_ref[...]
    one_ref[rows:, :] = b_ref[...]
    two_ref[:rows, :] = c_ref[...]
    two_ref[rows:, :] = d_ref[...]


def join(blocks):
    rows = blocks[0].shape[0]
    out = jax.ShapeDtypeStruct((2 * rows, 128), BF)
    return pl.pallas_call(join_body, out_shape=[out] * 2, name="join")(*blocks)


def load_piece(ref, k):
    at = pl.multiple_of(k * PIECE, PIECE)
    half = KEYS // 2
    pair = ref[pl.ds(at + KEYS, half), :]
    left = jnp.concatenate([ref[pl.ds(at, half), :], pair], axis=1)
    right = jnp.concatenate([ref[pl.ds(at + half, half), :], pair], axis=1)
    value = [ref[pl.ds(at + KEYS + half + 128 * c, 128), :] for c in range(4)]
    return left, right, jnp.concatenate(value, axis=1)


def own_body(kpos_ref, qpos_ref, low_ref, high_ref, kv_ref, *refs):
    m_ref, l_ref, acc_ref = refs[-3:]
    tile = 256
    half = KEYS // 2
    pieces = [load_piece(kv_ref, k) for k in range(2)]
    lefts = [pieces[0][0], pieces[0][1], pieces[1][0], pieces[1][1]]
    value = jnp.concatenate([pieces[0][2], pieces[1][2]], axis=1)
    for part in range(low_ref.shape[1] // tile):
        cols = slice(part * tile, (part + 1) * tile)
        scores = []
        for k, left in enumerate(lefts):
            s = dot(left, (high_ref if k % 2 else low_ref)[:, cols])
            allowed = kpos_ref[k * half : (k + 1) * half, :] <= qpos_ref[:, cols]
            scores.append(jnp.where(allowed, s, -1e30))
        peaks = [jnp.max(s, axis=0, keepdims=True) for s in scores]
        m = jnp.maximum(jnp.maximum(peaks[0], peaks[1]), jnp.maximum(peaks[2], peaks[3]))
        base = m * SCALE2
        probs = [jnp.exp2(s * SCALE2 - base) for s in scores]
        sums = [jnp.sum(p, axis=0, keepdims=True) for p in probs]
        m_ref[:, cols] = m
        l_ref[:, cols] = (sums[0] + sums[1]) + (sums[2] + sums[3])
        acc_ref[:, cols] = dot(value, jnp.concatenate([p.astype(BF) for p in probs], axis=0))


def own_attention(low, high, kv, positions):
    rows = low.shape[1]
    thin = jax.ShapeDtypeStruct((1, rows), F32)
    vmem = pl.BlockSpec(memory_space=pltpu.VMEM)
    return pl.pallas_call(
        own_body,
        in_specs=[vmem] * 5,
        out_specs=[vmem] * 3,
        out_shape=[thin, thin, jax.ShapeDtypeStruct((VDIM, rows), F32)],
        cost_estimate=pl.CostEstimate(
            flops=2 * rows * rows * 384, bytes_accessed=4 << 20, transcendentals=rows * rows
        ),
        name="own_attention",
    )(positions.reshape(-1, 1), positions.reshape(1, -1), low, high, kv)


def more_body(arrays, first, final, flags_ref, low_ref, high_ref, *refs):
    pieces = refs[:arrays]
    m_in, l_in, acc_in = refs[arrays : arrays + 3]
    keys_ref, sems = refs[-2:]
    m_ref, l_ref, acc_ref = refs[-5:-2]
    size = pieces[0].shape[0]

    def fetch(ref, number):
        target = keys_ref.at[pl.ds(pl.multiple_of(number * size, size), size)]
        return pltpu.make_async_copy(ref, target, sems.at[number])

    for number, ref in enumerate(pieces):
        fetch(ref, number).start()
    tile = 256
    tiles = low_ref.shape[1] // tile

    def start():
        m_ref[...] = m_in[...]
        l_ref[...] = l_in[...]
        acc_ref[...] = acc_in[...]

    def score(piece, t):
        cols = slice(t * tile, (t + 1) * tile)
        return dot(piece[0], low_ref[:, cols]), dot(piece[1], high_ref[:, cols])

    def over(step, wait):
        def array(number, _):
            if wait:
                fetch(pieces[0], number).wait()

            def one(k, _):
                @pl.when(flags_ref[first + 2 * number + k] != 0)
                def _():
                    step(2 * number + k)

                return 0

            lax.fori_loop(0, 2, one, 0)
            return 0

        lax.fori_loop(0, arrays, array, 0)

    def weigh(s, t):
        cols = slice(t * tile, (t + 1) * tile)
        base = m_ref[:, cols] * SCALE2
        p = jnp.exp2(s[0] * SCALE2 - base)
        q = jnp.exp2(s[1] * SCALE2 - base)
        l_ref[:, cols] += jnp.sum(p, axis=0, keepdims=True) + jnp.sum(q, axis=0, keepdims=True)
        return jnp.concatenate([p.astype(BF), q.astype(BF)], axis=0)

    def gather(piece, probs, t):
        cols = slice(t * tile, (t + 1) * tile)
        acc_ref[:, cols] += dot(piece[2], probs)

    def quick(k):
        block = [load_piece(keys_ref, 2 * k), load_piece(keys_ref, 2 * k + 1)]
        steps = [(piece, t) for piece in block for t in range(tiles)]
        s = score(*steps[0])
        before = None
        for i, (_, t) in enumerate(steps):
            after = score(*steps[i + 1]) if i + 1 < len(steps) else None
            if before is not None:
                gather(steps[i - 1][0], before, steps[i - 1][1])
            before = weigh(s, t)
            s = after
        gather(steps[-1][0], before, steps[-1][1])

    def careful(k):
        def one(i, _):
            piece = load_piece(keys_ref, 2 * k + i // tiles)
            cols = pl.ds(pl.multiple_of((i % tiles) * tile, tile), tile)
            p = dot(piece[0], low_ref[:, cols])
            q = dot(piece[1], high_ref[:, cols])
            before = m_ref[:, cols]
            peak = jnp.maximum(jnp.max(p, axis=0, keepdims=True), jnp.max(q, axis=0, keepdims=True))
            m = jnp.maximum(before, peak)
            alpha = jnp.exp2((before - m) * SCALE2)
            p = jnp.exp2(p * SCALE2 - m * SCALE2)
            q = jnp.exp2(q * SCALE2 - m * SCALE2)
            m_ref[:, cols] = m
            total = jnp.sum(p, axis=0, keepdims=True) + jnp.sum(q, axis=0, keepdims=True)
            l_ref[:, cols] = l_ref[:, cols] * alpha + total
            probs = jnp.concatenate([p.astype(BF), q.astype(BF)], axis=0)
            acc_ref[:, cols] = acc_ref[:, cols] * alpha + dot(piece[2], probs)
            return 0

        lax.fori_loop(0, 2 * tiles, one, 0)

    start()
    over(quick, True)
    safe = jnp.where(l_ref[...] < LIMIT, 0.0, 1.0)

    @pl.when(jnp.max(safe) > 0.0)
    def _():
        start()
        over(careful, False)

    if final:
        done = (acc_ref[...] / l_ref[...]).astype(BF)
        for b in range(4):
            refs[arrays + 3 + b][...] = done[:, 256 * b : 256 * (b + 1)]


def more_attention(low, high, arrays, flags, first, state, final=False):
    rows = low.shape[1]
    keys = 4 * len(arrays) * KEYS
    shapes = [(1, rows), (1, rows), (VDIM, rows)]
    if final:
        out_shape = [jax.ShapeDtypeStruct((VDIM, rows // 4), BF)] * 4
        scratch = [pltpu.VMEM(s, F32) for s in shapes]
    else:
        out_shape = [jax.ShapeDtypeStruct(s, F32) for s in shapes]
        scratch = []
    vmem = pl.BlockSpec(memory_space=pltpu.VMEM)
    count = len(arrays)
    scratch += [
        pltpu.VMEM((count * arrays[0].shape[0], 128), BF),
        pltpu.SemaphoreType.DMA((count,)),
    ]
    return pl.pallas_call(
        functools.partial(more_body, count, first, final),
        in_specs=[pl.BlockSpec(memory_space=pltpu.SMEM), vmem, vmem]
        + [pl.BlockSpec(memory_space=pl.ANY)] * count
        + [vmem] * 3,
        out_specs=[vmem] * len(out_shape),
        out_shape=out_shape,
        scratch_shapes=scratch,
        cost_estimate=pl.CostEstimate(
            flops=rows * keys * 384, bytes_accessed=4 << 20, transcendentals=rows * keys
        ),
        name="more_attention",
    )(flags, low, high, *arrays, *state)


def project_body(*refs):
    left = jnp.concatenate([r[...] for r in refs[:4]], axis=0)
    right = jnp.concatenate([r[...] for r in refs[4:8]], axis=0)
    mine, other = refs[8:]
    result = dot(left, right, (((0,), (0,)), ((), ())))
    rows = mine.shape[0]
    mine[...] = result[:rows]
    other[...] = result[rows:].astype(BF)


def project(attended, blocks):
    rows = attended[0].shape[1] // 2
    width = blocks[0].shape[1]
    return pl.pallas_call(
        project_body,
        grid=(width // 512,),
        in_specs=[whole(a.shape) for a in attended] + [columns(128)] * 4,
        out_specs=[columns(rows)] * 2,
        out_shape=[
            jax.ShapeDtypeStruct((rows, width), F32),
            jax.ShapeDtypeStruct((rows, width), BF),
        ],
        name="project",
    )(*attended, *blocks)


def angles(positions):
    half = ROPE // 2
    freq = 1.0 / THETA ** (jnp.arange(half, dtype=F32) * 2.0 / ROPE)
    return positions.astype(F32), freq


def turn(values):
    half = ROPE // 2
    return jnp.concatenate([-values[:, half:], values[:, :half]], axis=-1)


LINE = (0, 1, -1, 2)


def sources():
    near = [(d, 0) for d in LINE]
    wide = [(a, b) for b in (1, -1) for a in LINE]
    far = [(a, 2) for a in LINE]
    return near + wide + far


def own_block(query_latent, kv_latent, rope_key, query_gain, kv_gain):
    local = query_latent.shape[0]
    first = (lax.axis_index("ep") * 8 + lax.axis_index("tp")) * local
    place, freq = angles(first + jnp.arange(local, dtype=jnp.int32))
    angle = place[:, None] * freq[None, :]
    angle = jnp.concatenate([angle, angle], axis=-1)
    key_in = rope_key.astype(F32)
    key_rot = (key_in * jnp.cos(angle) + turn(key_in) * jnp.sin(angle)).astype(BF)
    return prepare(query_latent, kv_latent, key_rot, query_gain, kv_gain)


def mixer(query_latent, query_nope_w, query_rope_w, key_up_w, value_up_w, output_w, block):
    local = query_latent.shape[0]
    group = local * 8
    ep = lax.axis_index("ep")
    tp = lax.axis_index("tp")
    z, x = ep // 4, ep % 4
    y, core = tp // 2, tp % 2
    behind, ahead, far = ring(block, along_y)
    outputs = (output_w, *ring(output_w, along_y))
    blocks = [block, swap(block), behind, swap(ahead), ahead, swap(behind), far, swap(far)]
    turned = 1 - 2 * core
    chips = (y + turned * np.array([0, -1, 1, 2], np.int32)) % 4
    one = np.array([s[0] for s in sources()], np.int32)
    two = np.array([s[1] for s in sources()], np.int32)
    dz = jnp.where(core == 0, one, two)
    dx = jnp.where(core == 0, two, one)
    flags = (((z - dz) % 4) * 4 + (x - dx) % 4 < ep).astype(jnp.int32)
    order = chips[:, None] * 2 + (core ^ np.array([[0, 1]], np.int32))
    inside = (order.reshape(8, 1) * local + np.arange(local, dtype=np.int32)[None, :]).reshape(-1)
    place, freq = angles(ep * group + inside)
    angle = freq[:, None] * place[None, :]
    turns = jnp.cos(angle), jnp.sin(angle)
    kv, low, high = heads(blocks, key_up_w, value_up_w, query_nope_w, query_rope_w, *turns)
    one, two = join([kv, *ring(kv, along_one)])
    behind, ahead, far = ring_halves(one, two, along_two)
    state = own_attention(low, high, kv, inside)
    state = more_attention(low, high, (one, two), flags, 0, state)
    state = more_attention(low, high, (*behind, *ahead), flags, 4, state)
    attended = more_attention(low, high, far, flags, 12, state, final=True)
    attended = (
        attended[0],
        send(attended[2], along_y(1)),
        send(attended[1], along_y(-1)),
        send(attended[3], along_y(2)),
    )
    mine, other = project(attended, outputs)
    return add((mine, swap(other)))[0]


def per_device(
    query_latent,
    kv_latent,
    rope_key,
    query_gain,
    kv_gain,
    query_nope_w,
    query_rope_w,
    key_up_w,
    value_up_w,
    output_w,
    expert_in,
    moe_gain,
    routes,
    route_weight,
    gate_w,
    up_w,
    down_w,
):
    block = own_block(query_latent, kv_latent, rope_key, query_gain, kv_gain)
    mixer_out = mixer(
        query_latent, query_nope_w, query_rope_w, key_up_w, value_up_w, output_w, block
    )
    expert_out = experts_half(
        expert_in, moe_gain, routes, route_weight, gate_w, up_w, down_w
    )
    return (mixer_out, expert_out)


def solution(mesh):
    placed = (
        P(("ep", "tp"), None),
        P(("ep", "tp"), None),
        P(("ep", "tp"), None),
        P(),
        P(),
        P(None, "tp"),
        P(None, "tp"),
        P(None, "tp"),
        P(None, "tp"),
        P("tp", None),
        P(("ep", "tp"), None),
        P(),
        P(("ep", "tp"), None),
        P(("ep", "tp"), None),
        P("ep", None, "tp"),
        P("ep", None, "tp"),
        P("ep", "tp", None),
    )
    return jax.shard_map(
        per_device,
        mesh=mesh,
        in_specs=placed,
        out_specs=(P(("ep", "tp"), None), P(("ep", "tp"), None)),
        check_vma=False,
    )
```

```python
import functools
import math

import jax
import jax.numpy as jnp
import numpy as np
from jax import lax
from jax.experimental import pallas as pl
from jax.experimental.pallas import tpu as pltpu
from jax.sharding import PartitionSpec as P


NOPE = 128
ROPE = 64
VDIM = 128
THETA = 10000.0
CHUNK = 24
HALF = 12
CAP = 10
BF = jnp.bfloat16
F32 = jnp.float32
LOG2E = 1.4426950408889634


def dot(a, b, dims=(((1,), (0,)), ((), ()))):
    return lax.dot_general(a, b, dims, preferred_element_type=F32)


def pairs(move):
    result = []
    for device in range(128):
        ep, tp = divmod(device, 8)
        z, x, y, core = ep // 4, ep % 4, tp // 2, tp % 2
        dz, dx, dy, dc = move(core)
        ep = ((z + dz) % 4) * 4 + (x + dx) % 4
        tp = ((y + dy) % 4) * 2 + (core ^ dc)
        result.append((device, ep * 8 + tp))
    return result


def send(a, move):
    return lax.ppermute(a, ("ep", "tp"), pairs(move))


def swap(a):
    return send(a, lambda core: (0, 0, 0, 1))


def along_y(d):
    return lambda core: (0, 0, -d if core else d, 0)


def plain_y(d):
    return lambda core: (0, 0, d, 0)


def along_one(d):
    return lambda core: (0, d, 0, 0) if core else (d, 0, 0, 0)


def along_two(d):
    return lambda core: (d, 0, 0, 0) if core else (0, d, 0, 0)


def ring(block, along):
    behind = send(block, along(1))
    ahead = send(block, along(-1))
    far = send(behind, along(1))
    return behind, ahead, far


def ring_halves(one, two, along):
    one_behind = send(one, along(1))
    two_ahead = send(two, along(-1))
    two_behind = send(two, along(1))
    one_ahead = send(one, along(-1))
    one_far = send(one_behind, along(1))
    two_far = send(two_ahead, along(-1))
    return (one_behind, two_behind), (one_ahead, two_ahead), (one_far, two_far)


def slots_of(route, rank):
    return (route >> 1) * CHUNK + (route & 1) * HALF + rank


def upright(row):
    count = row.shape[1]
    i = lax.broadcasted_iota(jnp.int32, (count, count), 0)
    j = lax.broadcasted_iota(jnp.int32, (count, count), 1)
    spread = jnp.where(i == j, row.astype(F32), 0.0)
    return jnp.sum(spread, axis=1, keepdims=True).astype(jnp.int32)


def dispatch_body(x_ref, gain_ref, row_ref, out_ref):
    floats = x_ref[...].astype(F32)
    center = floats - jnp.mean(floats, axis=-1, keepdims=True)
    variance = jnp.mean(center * center, axis=-1, keepdims=True)
    normed = (center * lax.rsqrt(variance + 1e-05) * gain_ref[...][None, :]).astype(BF)
    count = x_ref.shape[0]
    cols = [upright(row_ref[k : k + 1, :]) for k in range(2)]
    j = lax.broadcasted_iota(jnp.int32, (count, count), 0)
    i = lax.broadcasted_iota(jnp.int32, (count, count), 1)
    earlier = j < i
    total = out_ref.shape[0]
    number = lax.broadcasted_iota(jnp.int32, (total, count), 0)
    select = None
    for k in range(2):
        mine = row_ref[k : k + 1, :]
        same = (cols[0] == mine) | (cols[1] == mine)
        rank = jnp.sum(jnp.where(same & earlier, 1.0, 0.0), axis=0, keepdims=True)
        hit = number == slots_of(mine, rank.astype(jnp.int32))
        select = hit if select is None else select | hit
    pick = jnp.where(select, 1.0, 0.0).astype(BF)
    out_ref[...] = dot(pick, normed).astype(BF)


def dispatch(x, gain, routes):
    return pl.pallas_call(
        dispatch_body,
        out_shape=jax.ShapeDtypeStruct((16 * CHUNK, x.shape[1]), BF),
        name="dispatch",
    )(x, gain, routes.T)


def combine_body(back_ref, row_ref, w_ref, out_ref):
    count = row_ref.shape[1]
    i = lax.broadcasted_iota(jnp.int32, (count, count), 0)
    j = lax.broadcasted_iota(jnp.int32, (count, count), 1)
    earlier = j < i
    total = back_ref.shape[0]
    number = lax.broadcasted_iota(jnp.int32, (count, total), 1)
    weight = w_ref[...]
    weight = weight / jnp.sum(weight, axis=-1, keepdims=True)
    back = back_ref[...]
    result = None
    for k in range(2):
        mine = upright(row_ref[k : k + 1, :])
        same = (row_ref[0:1, :] == mine) | (row_ref[1:2, :] == mine)
        rank = jnp.sum(jnp.where(same & earlier, 1.0, 0.0), axis=1, keepdims=True)
        hit = number == slots_of(mine, rank.astype(jnp.int32))
        pick = jnp.where(hit, 1.0, 0.0).astype(BF)
        term = dot(pick, back) * weight[:, k : k + 1]
        result = term if result is None else result + term
    out_ref[...] = result.astype(BF)


def combine(back, routes, route_weight):
    return pl.pallas_call(
        combine_body,
        out_shape=jax.ShapeDtypeStruct((routes.shape[0], back.shape[1]), BF),
        name="combine",
    )(back, routes.T, route_weight)


def packing(flip):
    rows, cols = 16 * 2 * CAP, 16 * CHUNK
    shape = (cols, rows) if flip else (rows, cols)
    r = lax.broadcasted_iota(jnp.int32, shape, flip)
    c = lax.broadcasted_iota(jnp.int32, shape, 1 - flip)
    per = 16 * CAP
    slot = ((r % per) // CAP) * CHUNK + (r // per) * HALF + r % CAP
    return (slot == c).astype(BF)


def pack_body(pick_ref, x_ref, one_ref, two_ref):
    rows = one_ref.shape[0]
    packed = dot(pick_ref[...], x_ref[...]).astype(BF)
    one_ref[...] = packed[:rows]
    two_ref[...] = packed[rows:]


def columns(rows, width=512):
    return pl.BlockSpec((rows, width), lambda n: (0, n))


def whole(shape):
    return pl.BlockSpec(shape, lambda n: (0,) * len(shape))


def pack(pick, arrived):
    rows, width = arrived.shape
    half = pick.shape[0] // 2
    return pl.pallas_call(
        pack_body,
        grid=(2,),
        in_specs=[whole(pick.shape), columns(rows, width // 2)],
        out_specs=[columns(half, width // 2)] * 2,
        out_shape=[jax.ShapeDtypeStruct((half, width), BF)] * 2,
        name="pack",
    )(pick, arrived)


def unpack_body(pick_ref, *refs):
    out_ref = refs[-1]
    halves = []
    for k in range(2):
        a, b, c = refs[k:6:2]
        halves.append((a[...].astype(F32) + b[...].astype(F32) + c[...].astype(F32)).astype(BF))
    summed = jnp.concatenate(halves, axis=0)
    out_ref[...] = dot(pick_ref[...], summed).astype(BF)


def unpack(pick, *terms):
    rows, width = terms[0][0].shape
    return pl.pallas_call(
        unpack_body,
        grid=(2,),
        in_specs=[whole(pick.shape)] + [columns(rows, width // 2)] * 6,
        out_specs=columns(pick.shape[0], width // 2),
        out_shape=jax.ShapeDtypeStruct((pick.shape[0], width), BF),
        name="unpack",
    )(pick, *[a for pair in terms for a in pair])


def add_body(*refs):
    count = len(refs) // 3
    for k in range(count):
        a, b = refs[2 * k], refs[2 * k + 1]
        refs[2 * count + k][...] = (a[...].astype(F32) + b[...].astype(F32)).astype(BF)


def add(*pairs):
    rows, width = pairs[0][0].shape
    count = len(pairs)
    block = pl.BlockSpec((rows // 2, width), lambda n: (n, 0))
    return pl.pallas_call(
        add_body,
        grid=(2,),
        in_specs=[block] * 2 * count,
        out_specs=[block] * count,
        out_shape=[jax.ShapeDtypeStruct((rows, width), BF)] * count,
        name="add",
    )(*[a for pair in pairs for a in pair])


def ffn_body(count, *refs):
    xs = refs[: 2 * count]
    sources = refs[2 * count : 2 * count + 6]
    outs = refs[2 * count + 6 : 4 * count + 6]
    gates, uppers, downs, sems = refs[4 * count + 6 :]
    copies = []
    for expert in range(2):
        for half in range(2):
            for k, target in enumerate((gates, uppers, downs)):
                number = len(copies)
                copies.append(
                    pltpu.make_async_copy(
                        sources[half * 3 + k].at[expert],
                        target.at[expert * 2 + half],
                        sems.at[number],
                    )
                )
    for copy in copies:
        copy.start()
    rows = xs[0].shape[0]
    for expert in range(2):
        mine = xs[expert::2]
        x = mine[0][...] if count == 1 else jnp.concatenate([r[...] for r in mine], axis=0)
        hidden = []
        for half in range(2):
            at = expert * 2 + half
            for k in range(3):
                copies[at * 3 + k].wait()
            gate = jnp.minimum(dot(x, gates[at]), 7.0)
            upper = jnp.clip(dot(x, uppers[at]), -7.0, 7.0)
            hidden.append((gate * jax.nn.sigmoid(1.702 * gate) * (upper + 1.0)).astype(BF))
        total = dot(hidden[0], downs[expert * 2]) + dot(hidden[1], downs[expert * 2 + 1])
        total = total.astype(BF)
        for k in range(count):
            outs[2 * k + expert][...] = total[k * rows : (k + 1) * rows]


def ffn(weights, *xs):
    rows, width = xs[0][0].shape
    count = len(xs)
    inner = weights[0].shape[2]
    vmem = pl.BlockSpec(memory_space=pltpu.VMEM)
    out = jax.ShapeDtypeStruct((rows, width), BF)
    outs = pl.pallas_call(
        functools.partial(ffn_body, count),
        in_specs=[vmem] * 2 * count + [pl.BlockSpec(memory_space=pl.ANY)] * 6,
        out_specs=[vmem] * 2 * count,
        out_shape=[out] * 2 * count,
        scratch_shapes=[
            pltpu.VMEM((4, width, inner), BF),
            pltpu.VMEM((4, width, inner), BF),
            pltpu.VMEM((4, inner, width), BF),
            pltpu.SemaphoreType.DMA((12,)),
        ],
        cost_estimate=pl.CostEstimate(
            flops=12 * rows * count * width * 512, bytes_accessed=16 << 20, transcendentals=0
        ),
        name="ffn",
    )(*[a for pair in xs for a in pair], *weights)
    return [tuple(outs[2 * k : 2 * k + 2]) for k in range(count)]


def experts_half(
    expert_in, moe_gain, routes, route_weight, gate_w, up_w, down_w
):
    width = expert_in.shape[1]
    outgoing = dispatch(expert_in, moe_gain, routes)
    weights = (gate_w, up_w, down_w, swap(gate_w), swap(up_w), swap(down_w))
    arrived = lax.all_to_all(
        outgoing.reshape(16, CHUNK, width), "ep", split_axis=0, concat_axis=0, tiled=True
    ).reshape(16 * CHUNK, width)
    own = pack(packing(0), arrived)
    below, above, far = ring_halves(*own, plain_y)
    (below0, above1), own_out = ffn(weights, (below[0], above[1]), own)
    from_above0 = send(below0, plain_y(-1))
    from_below1 = send(above1, plain_y(1))
    (far0, far1), (above0, below1) = ffn(weights, far, (above[0], below[1]))
    far0 = send(far0, plain_y(1))
    far1 = send(far1, plain_y(-1))
    above0, below1 = add((above0, far0), (below1, far1))
    from_below0 = send(above0, plain_y(1))
    from_above1 = send(below1, plain_y(-1))
    back = unpack(packing(1), own_out, (from_below0, from_below1), (from_above0, from_above1))
    back = lax.all_to_all(
        back.reshape(16, CHUNK, width), "ep", split_axis=0, concat_axis=0, tiled=True
    ).reshape(16 * CHUNK, width)
    return combine(back, routes, route_weight)


SCALE2 = LOG2E / math.sqrt(NOPE + ROPE)
QLAT = 768
KVLAT = 512
LATENT = 1536
KEYS = 512
PIECE = KEYS + KEYS // 2 + 4 * VDIM
NT = (((1,), (1,)), ((), ()))
LIMIT = 2.0**80


def prepare_body(q_ref, kv_ref, rot_ref, qg_ref, kvg_ref, out_ref):
    for ref, gain, at in ((q_ref, qg_ref, 0), (kv_ref, kvg_ref, QLAT)):
        floats = ref[...].astype(F32)
        square = jnp.mean(floats * floats, axis=-1, keepdims=True)
        normed = floats * lax.rsqrt(square + 1e-06) * gain[...][None, :]
        out_ref[:, at : at + ref.shape[1]] = normed.astype(BF)
    rot = rot_ref[...]
    both = jnp.concatenate([rot, jnp.zeros_like(rot)], axis=1)
    out_ref[:, QLAT + KVLAT : QLAT + KVLAT + 128] = both
    out_ref[:, QLAT + KVLAT + 128 :] = jnp.zeros((rot.shape[0], 128), BF)


def prepare(query_latent, kv_latent, key_rot, query_gain, kv_gain):
    return pl.pallas_call(
        prepare_body,
        out_shape=jax.ShapeDtypeStruct((query_latent.shape[0], LATENT), BF),
        name="prepare",
    )(query_latent, kv_latent, key_rot, query_gain, kv_gain)


def heads_body(*refs):
    blocks = refs[:8]
    key_ref, value_ref, nope_ref, rope_ref, cos_ref, sin_ref = refs[8:14]
    kv_ref, low_ref, high_ref = refs[14:]
    kv = jnp.concatenate([r[:, QLAT : QLAT + KVLAT] for r in blocks], axis=0)
    keys = dot(kv, key_ref[...]).astype(BF)
    values = dot(value_ref[...].T, kv, NT).astype(BF)
    rots = jnp.concatenate(
        [r[:, QLAT + KVLAT : QLAT + KVLAT + 128] for r in blocks], axis=0
    ).astype(F32)
    half = KEYS // 2
    for k in range(2):
        at = k * KEYS
        to = k * PIECE
        pair = rots[at : at + half] + pltpu.roll(rots[at + half : at + KEYS], ROPE, 1)
        kv_ref[to : to + KEYS, :] = keys[at : at + KEYS]
        kv_ref[to + KEYS : to + KEYS + half, :] = pair.astype(BF)
        for c in range(4):
            row = to + KEYS + half + 128 * c
            kv_ref[row : row + 128, :] = values[:, at + 128 * c : at + 128 * (c + 1)]
    query_in = jnp.concatenate([r[:, :QLAT] for r in blocks], axis=0)
    query = dot(jnp.concatenate([nope_ref[...].T, rope_ref[...]], axis=0), query_in, NT)
    first = query[NOPE : NOPE + ROPE // 2]
    second = query[NOPE + ROPE // 2 :]
    cosine = cos_ref[...]
    sine = sin_ref[...]
    rot = jnp.concatenate([first * cosine - second * sine, second * cosine + first * sine], axis=0)
    nope = query[:NOPE].astype(BF)
    rot = rot.astype(BF)
    blank = jnp.zeros_like(rot)
    low_ref[...] = jnp.concatenate([nope, rot, blank], axis=0)
    high_ref[...] = jnp.concatenate([nope, blank, rot], axis=0)


def heads(blocks, key_w, value_w, nope_w, rope_w, cosine, sine):
    rows = 8 * blocks[0].shape[0]
    query = jax.ShapeDtypeStruct((256, rows), BF)
    return pl.pallas_call(
        heads_body,
        out_shape=[jax.ShapeDtypeStruct((2 * PIECE, 128), BF), query, query],
        cost_estimate=pl.CostEstimate(
            flops=2 * rows * (QLAT * 192 + KVLAT * 256), bytes_accessed=6 << 20, transcendentals=0
        ),
        name="heads",
    )(*blocks, key_w, value_w, nope_w, rope_w.T, cosine, sine)


def join_body(a_ref, b_ref, c_ref, d_ref, one_ref, two_ref):
    rows = a_ref.shape[0]
    one_ref[:rows, :] = a_ref[...]
    one_ref[rows:, :] = b_ref[...]
    two_ref[:rows, :] = c_ref[...]
    two_ref[rows:, :] = d_ref[...]


def join(blocks):
    rows = blocks[0].shape[0]
    out = jax.ShapeDtypeStruct((2 * rows, 128), BF)
    return pl.pallas_call(join_body, out_shape=[out] * 2, name="join")(*blocks)


def load_piece(ref, k):
    at = pl.multiple_of(k * PIECE, PIECE)
    half = KEYS // 2
    pair = ref[pl.ds(at + KEYS, half), :]
    left = jnp.concatenate([ref[pl.ds(at, half), :], pair], axis=1)
    right = jnp.concatenate([ref[pl.ds(at + half, half), :], pair], axis=1)
    value = [ref[pl.ds(at + KEYS + half + 128 * c, 128), :] for c in range(4)]
    return left, right, jnp.concatenate(value, axis=1)


def own_body(kpos_ref, qpos_ref, low_ref, high_ref, kv_ref, *refs):
    m_ref, l_ref, acc_ref = refs[-3:]
    tile = 256
    half = KEYS // 2
    pieces = [load_piece(kv_ref, k) for k in range(2)]
    lefts = [pieces[0][0], pieces[0][1], pieces[1][0], pieces[1][1]]
    value = jnp.concatenate([pieces[0][2], pieces[1][2]], axis=1)

    def one(part, _):
        cols = pl.ds(pl.multiple_of(part * tile, tile), tile)
        scores = []
        for k, left in enumerate(lefts):
            s = dot(left, (high_ref if k % 2 else low_ref)[:, cols])
            allowed = kpos_ref[k * half : (k + 1) * half, :] <= qpos_ref[:, cols]
            scores.append(jnp.where(allowed, s, -1e30))
        peaks = [jnp.max(s, axis=0, keepdims=True) for s in scores]
        m = jnp.maximum(jnp.maximum(peaks[0], peaks[1]), jnp.maximum(peaks[2], peaks[3]))
        base = m * SCALE2
        probs = [jnp.exp2(s * SCALE2 - base) for s in scores]
        sums = [jnp.sum(p, axis=0, keepdims=True) for p in probs]
        m_ref[:, cols] = m
        l_ref[:, cols] = (sums[0] + sums[1]) + (sums[2] + sums[3])
        acc_ref[:, cols] = dot(value, jnp.concatenate([p.astype(BF) for p in probs], axis=0))
        return 0

    lax.fori_loop(0, low_ref.shape[1] // tile, one, 0)


def own_attention(low, high, kv, positions):
    rows = low.shape[1]
    thin = jax.ShapeDtypeStruct((1, rows), F32)
    vmem = pl.BlockSpec(memory_space=pltpu.VMEM)
    return pl.pallas_call(
        own_body,
        in_specs=[vmem] * 5,
        out_specs=[vmem] * 3,
        out_shape=[thin, thin, jax.ShapeDtypeStruct((VDIM, rows), F32)],
        cost_estimate=pl.CostEstimate(
            flops=2 * rows * rows * 384, bytes_accessed=4 << 20, transcendentals=rows * rows
        ),
        name="own_attention",
    )(positions.reshape(-1, 1), positions.reshape(1, -1), low, high, kv)


def more_body(arrays, first, final, flags_ref, low_ref, high_ref, *refs):
    pieces = refs[:arrays]
    m_in, l_in, acc_in = refs[arrays : arrays + 3]
    keys_ref, sems = refs[-2:]
    m_ref, l_ref, acc_ref = refs[-5:-2]
    size = pieces[0].shape[0]

    def fetch(ref, number):
        target = keys_ref.at[pl.ds(pl.multiple_of(number * size, size), size)]
        return pltpu.make_async_copy(ref, target, sems.at[number])

    for number, ref in enumerate(pieces):
        fetch(ref, number).start()
    tile = 256
    tiles = low_ref.shape[1] // tile

    def start():
        m_ref[...] = m_in[...]
        l_ref[...] = l_in[...]
        acc_ref[...] = acc_in[...]

    def score(piece, t):
        cols = slice(t * tile, (t + 1) * tile)
        return dot(piece[0], low_ref[:, cols]), dot(piece[1], high_ref[:, cols])

    def over(step, wait):
        def array(number, _):
            if wait:
                fetch(pieces[0], number).wait()

            def one(k, _):
                @pl.when(flags_ref[first + 2 * number + k] != 0)
                def _():
                    step(2 * number + k)

                return 0

            lax.fori_loop(0, 2, one, 0)
            return 0

        lax.fori_loop(0, arrays, array, 0)

    def weigh(s, t):
        cols = slice(t * tile, (t + 1) * tile)
        base = m_ref[:, cols] * SCALE2
        p = jnp.exp2(s[0] * SCALE2 - base)
        q = jnp.exp2(s[1] * SCALE2 - base)
        l_ref[:, cols] += jnp.sum(p, axis=0, keepdims=True) + jnp.sum(q, axis=0, keepdims=True)
        return jnp.concatenate([p.astype(BF), q.astype(BF)], axis=0)

    def gather(piece, probs, t):
        cols = slice(t * tile, (t + 1) * tile)
        acc_ref[:, cols] += dot(piece[2], probs)

    def quick(k):
        block = [load_piece(keys_ref, 2 * k), load_piece(keys_ref, 2 * k + 1)]
        steps = [(piece, t) for piece in block for t in range(tiles)]
        s = score(*steps[0])
        before = None
        for i, (_, t) in enumerate(steps):
            after = score(*steps[i + 1]) if i + 1 < len(steps) else None
            if before is not None:
                gather(steps[i - 1][0], before, steps[i - 1][1])
            before = weigh(s, t)
            s = after
        gather(steps[-1][0], before, steps[-1][1])

    def careful(k):
        def one(i, _):
            piece = load_piece(keys_ref, 2 * k + i // tiles)
            cols = pl.ds(pl.multiple_of((i % tiles) * tile, tile), tile)
            p = dot(piece[0], low_ref[:, cols])
            q = dot(piece[1], high_ref[:, cols])
            before = m_ref[:, cols]
            peak = jnp.maximum(jnp.max(p, axis=0, keepdims=True), jnp.max(q, axis=0, keepdims=True))
            m = jnp.maximum(before, peak)
            alpha = jnp.exp2((before - m) * SCALE2)
            p = jnp.exp2(p * SCALE2 - m * SCALE2)
            q = jnp.exp2(q * SCALE2 - m * SCALE2)
            m_ref[:, cols] = m
            total = jnp.sum(p, axis=0, keepdims=True) + jnp.sum(q, axis=0, keepdims=True)
            l_ref[:, cols] = l_ref[:, cols] * alpha + total
            probs = jnp.concatenate([p.astype(BF), q.astype(BF)], axis=0)
            acc_ref[:, cols] = acc_ref[:, cols] * alpha + dot(piece[2], probs)
            return 0

        lax.fori_loop(0, 2 * tiles, one, 0)

    start()
    over(quick, True)
    safe = jnp.where(l_ref[...] < LIMIT, 0.0, 1.0)

    @pl.when(jnp.max(safe) > 0.0)
    def _():
        start()
        over(careful, False)

    if final:
        done = (acc_ref[...] / l_ref[...]).astype(BF)
        for b in range(4):
            refs[arrays + 3 + b][...] = done[:, 256 * b : 256 * (b + 1)]


def more_attention(low, high, arrays, flags, first, state, final=False):
    rows = low.shape[1]
    keys = 4 * len(arrays) * KEYS
    shapes = [(1, rows), (1, rows), (VDIM, rows)]
    if final:
        out_shape = [jax.ShapeDtypeStruct((VDIM, rows // 4), BF)] * 4
        scratch = [pltpu.VMEM(s, F32) for s in shapes]
    else:
        out_shape = [jax.ShapeDtypeStruct(s, F32) for s in shapes]
        scratch = []
    vmem = pl.BlockSpec(memory_space=pltpu.VMEM)
    count = len(arrays)
    scratch += [
        pltpu.VMEM((count * arrays[0].shape[0], 128), BF),
        pltpu.SemaphoreType.DMA((count,)),
    ]
    return pl.pallas_call(
        functools.partial(more_body, count, first, final),
        in_specs=[pl.BlockSpec(memory_space=pltpu.SMEM), vmem, vmem]
        + [pl.BlockSpec(memory_space=pl.ANY)] * count
        + [vmem] * 3,
        out_specs=[vmem] * len(out_shape),
        out_shape=out_shape,
        scratch_shapes=scratch,
        cost_estimate=pl.CostEstimate(
            flops=rows * keys * 384, bytes_accessed=4 << 20, transcendentals=rows * keys
        ),
        name="more_attention",
    )(flags, low, high, *arrays, *state)


def project_body(*refs):
    left = jnp.concatenate([r[...] for r in refs[:4]], axis=0)
    right = jnp.concatenate([r[...] for r in refs[4:8]], axis=0)
    mine, other = refs[8:]
    result = dot(left, right, (((0,), (0,)), ((), ())))
    rows = mine.shape[0]
    mine[...] = result[:rows]
    other[...] = result[rows:].astype(BF)


def project(attended, blocks):
    rows = attended[0].shape[1] // 2
    width = blocks[0].shape[1]
    return pl.pallas_call(
        project_body,
        grid=(width // 512,),
        in_specs=[whole(a.shape) for a in attended] + [columns(128)] * 4,
        out_specs=[columns(rows)] * 2,
        out_shape=[
            jax.ShapeDtypeStruct((rows, width), F32),
            jax.ShapeDtypeStruct((rows, width), BF),
        ],
        name="project",
    )(*attended, *blocks)


def angles(positions):
    half = ROPE // 2
    freq = 1.0 / THETA ** (jnp.arange(half, dtype=F32) * 2.0 / ROPE)
    return positions.astype(F32), freq


def turn(values):
    half = ROPE // 2
    return jnp.concatenate([-values[:, half:], values[:, :half]], axis=-1)


LINE = (0, 1, -1, 2)


def sources():
    near = [(d, 0) for d in LINE]
    wide = [(a, 1) for a in LINE[:2]] + [(a, -1) for a in LINE[2:]]
    more = [(a, 1) for a in LINE[2:]] + [(a, -1) for a in LINE[:2]]
    far = [(a, 2) for a in LINE]
    return near + wide + more + far


def own_block(query_latent, kv_latent, rope_key, query_gain, kv_gain):
    local = query_latent.shape[0]
    first = (lax.axis_index("ep") * 8 + lax.axis_index("tp")) * local
    place, freq = angles(first + jnp.arange(local, dtype=jnp.int32))
    angle = place[:, None] * freq[None, :]
    angle = jnp.concatenate([angle, angle], axis=-1)
    key_in = rope_key.astype(F32)
    key_rot = (key_in * jnp.cos(angle) + turn(key_in) * jnp.sin(angle)).astype(BF)
    return prepare(query_latent, kv_latent, key_rot, query_gain, kv_gain)


def mixer(query_latent, query_nope_w, query_rope_w, key_up_w, value_up_w, output_w, block):
    local = query_latent.shape[0]
    group = local * 8
    ep = lax.axis_index("ep")
    tp = lax.axis_index("tp")
    z, x = ep // 4, ep % 4
    y, core = tp // 2, tp % 2
    behind, ahead, far = ring(block, along_y)
    outputs = (output_w, *ring(output_w, along_y))
    blocks = [block, swap(block), behind, swap(ahead), ahead, swap(behind), far, swap(far)]
    turned = 1 - 2 * core
    chips = (y + turned * np.array([0, -1, 1, 2], np.int32)) % 4
    one = np.array([s[0] for s in sources()], np.int32)
    two = np.array([s[1] for s in sources()], np.int32)
    dz = jnp.where(core == 0, one, two)
    dx = jnp.where(core == 0, two, one)
    flags = (((z - dz) % 4) * 4 + (x - dx) % 4 < ep).astype(jnp.int32)
    order = chips[:, None] * 2 + (core ^ np.array([[0, 1]], np.int32))
    inside = (order.reshape(8, 1) * local + np.arange(local, dtype=np.int32)[None, :]).reshape(-1)
    place, freq = angles(ep * group + inside)
    angle = freq[:, None] * place[None, :]
    turns = jnp.cos(angle), jnp.sin(angle)
    kv, low, high = heads(blocks, key_up_w, value_up_w, query_nope_w, query_rope_w, *turns)
    one, two = join([kv, *ring(kv, along_one)])
    behind, ahead, far = ring_halves(one, two, along_two)
    state = own_attention(low, high, kv, inside)
    state = more_attention(low, high, (one, two), flags, 0, state)
    wide = behind[0], ahead[1]
    more = behind[1], ahead[0]
    state = more_attention(low, high, wide, flags, 4, state)
    state = more_attention(low, high, more, flags, 8, state)
    attended = more_attention(low, high, far, flags, 12, state, final=True)
    attended = (
        attended[0],
        send(attended[2], along_y(1)),
        send(attended[1], along_y(-1)),
        send(attended[3], along_y(2)),
    )
    mine, other = project(attended, outputs)
    return add((mine, swap(other)))[0]


def per_device(
    query_latent,
    kv_latent,
    rope_key,
    query_gain,
    kv_gain,
    query_nope_w,
    query_rope_w,
    key_up_w,
    value_up_w,
    output_w,
    expert_in,
    moe_gain,
    routes,
    route_weight,
    gate_w,
    up_w,
    down_w,
):
    block = own_block(query_latent, kv_latent, rope_key, query_gain, kv_gain)
    mixer_out = mixer(
        query_latent, query_nope_w, query_rope_w, key_up_w, value_up_w, output_w, block
    )
    expert_out = experts_half(
        expert_in, moe_gain, routes, route_weight, gate_w, up_w, down_w
    )
    return (mixer_out, expert_out)


def solution(mesh):
    placed = (
        P(("ep", "tp"), None),
        P(("ep", "tp"), None),
        P(("ep", "tp"), None),
        P(),
        P(),
        P(None, "tp"),
        P(None, "tp"),
        P(None, "tp"),
        P(None, "tp"),
        P("tp", None),
        P(("ep", "tp"), None),
        P(),
        P(("ep", "tp"), None),
        P(("ep", "tp"), None),
        P("ep", None, "tp"),
        P("ep", None, "tp"),
        P("ep", "tp", None),
    )
    return jax.shard_map(
        per_device,
        mesh=mesh,
        in_specs=placed,
        out_specs=(P(("ep", "tp"), None), P(("ep", "tp"), None)),
        check_vma=False,
    )
```

```python
import functools
import math

import jax
import jax.numpy as jnp
import numpy as np
from jax import lax
from jax.experimental import pallas as pl
from jax.experimental.pallas import tpu as pltpu
from jax.sharding import PartitionSpec as P


NOPE = 128
ROPE = 64
VDIM = 128
THETA = 10000.0
CHUNK = 24
HALF = 12
CAP = 10
BF = jnp.bfloat16
F32 = jnp.float32
LOG2E = 1.4426950408889634


def dot(a, b, dims=(((1,), (0,)), ((), ()))):
    return lax.dot_general(a, b, dims, preferred_element_type=F32)


def pairs(move):
    result = []
    for device in range(128):
        ep, tp = divmod(device, 8)
        z, x, y, core = ep // 4, ep % 4, tp // 2, tp % 2
        dz, dx, dy, dc = move(core)
        ep = ((z + dz) % 4) * 4 + (x + dx) % 4
        tp = ((y + dy) % 4) * 2 + (core ^ dc)
        result.append((device, ep * 8 + tp))
    return result


def send(a, move):
    return lax.ppermute(a, ("ep", "tp"), pairs(move))


def swap(a):
    return send(a, lambda core: (0, 0, 0, 1))


def along_y(d):
    return lambda core: (0, 0, -d if core else d, 0)


def plain_y(d):
    return lambda core: (0, 0, d, 0)


def along_one(d):
    return lambda core: (0, d, 0, 0) if core else (d, 0, 0, 0)


def along_two(d):
    return lambda core: (d, 0, 0, 0) if core else (0, d, 0, 0)


def ring(block, along):
    behind = send(block, along(1))
    ahead = send(block, along(-1))
    far = send(behind, along(1))
    return behind, ahead, far


def ring_halves(one, two, along):
    one_behind = send(one, along(1))
    two_ahead = send(two, along(-1))
    two_behind = send(two, along(1))
    one_ahead = send(one, along(-1))
    one_far = send(one_behind, along(1))
    two_far = send(two_ahead, along(-1))
    return (one_behind, two_behind), (one_ahead, two_ahead), (one_far, two_far)


def slots_of(route, rank):
    return (route >> 1) * CHUNK + (route & 1) * HALF + rank


def upright(row):
    count = row.shape[1]
    i = lax.broadcasted_iota(jnp.int32, (count, count), 0)
    j = lax.broadcasted_iota(jnp.int32, (count, count), 1)
    spread = jnp.where(i == j, row.astype(F32), 0.0)
    return jnp.sum(spread, axis=1, keepdims=True).astype(jnp.int32)


def dispatch_body(x_ref, gain_ref, row_ref, out_ref):
    floats = x_ref[...].astype(F32)
    center = floats - jnp.mean(floats, axis=-1, keepdims=True)
    variance = jnp.mean(center * center, axis=-1, keepdims=True)
    normed = (center * lax.rsqrt(variance + 1e-05) * gain_ref[...][None, :]).astype(BF)
    count = x_ref.shape[0]
    cols = [upright(row_ref[k : k + 1, :]) for k in range(2)]
    j = lax.broadcasted_iota(jnp.int32, (count, count), 0)
    i = lax.broadcasted_iota(jnp.int32, (count, count), 1)
    earlier = j < i
    total = out_ref.shape[0]
    number = lax.broadcasted_iota(jnp.int32, (total, count), 0)
    select = None
    for k in range(2):
        mine = row_ref[k : k + 1, :]
        same = (cols[0] == mine) | (cols[1] == mine)
        rank = jnp.sum(jnp.where(same & earlier, 1.0, 0.0), axis=0, keepdims=True)
        hit = number == slots_of(mine, rank.astype(jnp.int32))
        select = hit if select is None else select | hit
    pick = jnp.where(select, 1.0, 0.0).astype(BF)
    out_ref[...] = dot(pick, normed).astype(BF)


def dispatch(x, gain, routes):
    return pl.pallas_call(
        dispatch_body,
        out_shape=jax.ShapeDtypeStruct((16 * CHUNK, x.shape[1]), BF),
        name="dispatch",
    )(x, gain, routes.T)


def combine_body(back_ref, row_ref, w_ref, out_ref):
    count = row_ref.shape[1]
    i = lax.broadcasted_iota(jnp.int32, (count, count), 0)
    j = lax.broadcasted_iota(jnp.int32, (count, count), 1)
    earlier = j < i
    total = back_ref.shape[0]
    number = lax.broadcasted_iota(jnp.int32, (count, total), 1)
    weight = w_ref[...]
    weight = weight / jnp.sum(weight, axis=-1, keepdims=True)
    back = back_ref[...]
    result = None
    for k in range(2):
        mine = upright(row_ref[k : k + 1, :])
        same = (row_ref[0:1, :] == mine) | (row_ref[1:2, :] == mine)
        rank = jnp.sum(jnp.where(same & earlier, 1.0, 0.0), axis=1, keepdims=True)
        hit = number == slots_of(mine, rank.astype(jnp.int32))
        pick = jnp.where(hit, 1.0, 0.0).astype(BF)
        term = dot(pick, back) * weight[:, k : k + 1]
        result = term if result is None else result + term
    out_ref[...] = result.astype(BF)


def combine(back, routes, route_weight):
    return pl.pallas_call(
        combine_body,
        out_shape=jax.ShapeDtypeStruct((routes.shape[0], back.shape[1]), BF),
        name="combine",
    )(back, routes.T, route_weight)


def packing(flip):
    rows, cols = 16 * 2 * CAP, 16 * CHUNK
    shape = (cols, rows) if flip else (rows, cols)
    r = lax.broadcasted_iota(jnp.int32, shape, flip)
    c = lax.broadcasted_iota(jnp.int32, shape, 1 - flip)
    per = 16 * CAP
    slot = ((r % per) // CAP) * CHUNK + (r // per) * HALF + r % CAP
    return (slot == c).astype(BF)


def pack_body(pick_ref, x_ref, one_ref, two_ref):
    rows = one_ref.shape[0]
    packed = dot(pick_ref[...], x_ref[...]).astype(BF)
    one_ref[...] = packed[:rows]
    two_ref[...] = packed[rows:]


def columns(rows, width=512):
    return pl.BlockSpec((rows, width), lambda n: (0, n))


def whole(shape):
    return pl.BlockSpec(shape, lambda n: (0,) * len(shape))


def pack(pick, arrived):
    rows, width = arrived.shape
    half = pick.shape[0] // 2
    return pl.pallas_call(
        pack_body,
        grid=(2,),
        in_specs=[whole(pick.shape), columns(rows, width // 2)],
        out_specs=[columns(half, width // 2)] * 2,
        out_shape=[jax.ShapeDtypeStruct((half, width), BF)] * 2,
        name="pack",
    )(pick, arrived)


def unpack_body(pick_ref, *refs):
    out_ref = refs[-1]
    halves = []
    for k in range(2):
        a, b, c = refs[k:6:2]
        halves.append((a[...].astype(F32) + b[...].astype(F32) + c[...].astype(F32)).astype(BF))
    summed = jnp.concatenate(halves, axis=0)
    out_ref[...] = dot(pick_ref[...], summed).astype(BF)


def unpack(pick, *terms):
    rows, width = terms[0][0].shape
    return pl.pallas_call(
        unpack_body,
        grid=(2,),
        in_specs=[whole(pick.shape)] + [columns(rows, width // 2)] * 6,
        out_specs=columns(pick.shape[0], width // 2),
        out_shape=jax.ShapeDtypeStruct((pick.shape[0], width), BF),
        name="unpack",
    )(pick, *[a for pair in terms for a in pair])


def add_body(*refs):
    count = len(refs) // 3
    for k in range(count):
        a, b = refs[2 * k], refs[2 * k + 1]
        refs[2 * count + k][...] = (a[...].astype(F32) + b[...].astype(F32)).astype(BF)


def add(*pairs):
    rows, width = pairs[0][0].shape
    count = len(pairs)
    block = pl.BlockSpec((rows // 2, width), lambda n: (n, 0))
    return pl.pallas_call(
        add_body,
        grid=(2,),
        in_specs=[block] * 2 * count,
        out_specs=[block] * count,
        out_shape=[jax.ShapeDtypeStruct((rows, width), BF)] * count,
        name="add",
    )(*[a for pair in pairs for a in pair])


def ffn_body(count, *refs):
    xs = refs[: 2 * count]
    sources = refs[2 * count : 2 * count + 6]
    outs = refs[2 * count + 6 : 4 * count + 6]
    gates, uppers, downs, sems = refs[4 * count + 6 :]
    copies = []
    for expert in range(2):
        for half in range(2):
            for k, target in enumerate((gates, uppers, downs)):
                number = len(copies)
                copies.append(
                    pltpu.make_async_copy(
                        sources[half * 3 + k].at[expert],
                        target.at[expert * 2 + half],
                        sems.at[number],
                    )
                )
    for copy in copies:
        copy.start()
    rows = xs[0].shape[0]
    for expert in range(2):
        mine = xs[expert::2]
        x = mine[0][...] if count == 1 else jnp.concatenate([r[...] for r in mine], axis=0)
        hidden = []
        for half in range(2):
            at = expert * 2 + half
            for k in range(3):
                copies[at * 3 + k].wait()
            gate = jnp.minimum(dot(x, gates[at]), 7.0)
            upper = jnp.clip(dot(x, uppers[at]), -7.0, 7.0)
            hidden.append((gate * jax.nn.sigmoid(1.702 * gate) * (upper + 1.0)).astype(BF))
        total = dot(hidden[0], downs[expert * 2]) + dot(hidden[1], downs[expert * 2 + 1])
        total = total.astype(BF)
        for k in range(count):
            outs[2 * k + expert][...] = total[k * rows : (k + 1) * rows]


def ffn(weights, *xs):
    rows, width = xs[0][0].shape
    count = len(xs)
    inner = weights[0].shape[2]
    vmem = pl.BlockSpec(memory_space=pltpu.VMEM)
    out = jax.ShapeDtypeStruct((rows, width), BF)
    outs = pl.pallas_call(
        functools.partial(ffn_body, count),
        in_specs=[vmem] * 2 * count + [pl.BlockSpec(memory_space=pl.ANY)] * 6,
        out_specs=[vmem] * 2 * count,
        out_shape=[out] * 2 * count,
        scratch_shapes=[
            pltpu.VMEM((4, width, inner), BF),
            pltpu.VMEM((4, width, inner), BF),
            pltpu.VMEM((4, inner, width), BF),
            pltpu.SemaphoreType.DMA((12,)),
        ],
        cost_estimate=pl.CostEstimate(
            flops=12 * rows * count * width * 512, bytes_accessed=16 << 20, transcendentals=0
        ),
        name="ffn",
    )(*[a for pair in xs for a in pair], *weights)
    return [tuple(outs[2 * k : 2 * k + 2]) for k in range(count)]


def experts_half(
    expert_in, moe_gain, routes, route_weight, gate_w, up_w, down_w
):
    width = expert_in.shape[1]
    outgoing = dispatch(expert_in, moe_gain, routes)
    weights = (gate_w, up_w, down_w, swap(gate_w), swap(up_w), swap(down_w))
    arrived = lax.all_to_all(
        outgoing.reshape(16, CHUNK, width), "ep", split_axis=0, concat_axis=0, tiled=True
    ).reshape(16 * CHUNK, width)
    own = pack(packing(0), arrived)
    below, above, far = ring_halves(*own, plain_y)
    (below0, above1), own_out = ffn(weights, (below[0], above[1]), own)
    from_above0 = send(below0, plain_y(-1))
    from_below1 = send(above1, plain_y(1))
    (far0, far1), (above0, below1) = ffn(weights, far, (above[0], below[1]))
    far0 = send(far0, plain_y(1))
    far1 = send(far1, plain_y(-1))
    above0, below1 = add((above0, far0), (below1, far1))
    from_below0 = send(above0, plain_y(1))
    from_above1 = send(below1, plain_y(-1))
    back = unpack(packing(1), own_out, (from_below0, from_below1), (from_above0, from_above1))
    back = lax.all_to_all(
        back.reshape(16, CHUNK, width), "ep", split_axis=0, concat_axis=0, tiled=True
    ).reshape(16 * CHUNK, width)
    return combine(back, routes, route_weight)


SCALE2 = LOG2E / math.sqrt(NOPE + ROPE)
QLAT = 768
KVLAT = 512
LATENT = 1536
KEYS = 512
PIECE = KEYS + KEYS // 2 + 4 * VDIM
NT = (((1,), (1,)), ((), ()))
LIMIT = 2.0**80


def prepare_body(q_ref, kv_ref, rot_ref, qg_ref, kvg_ref, out_ref):
    for ref, gain, at in ((q_ref, qg_ref, 0), (kv_ref, kvg_ref, QLAT)):
        floats = ref[...].astype(F32)
        square = jnp.mean(floats * floats, axis=-1, keepdims=True)
        normed = floats * lax.rsqrt(square + 1e-06) * gain[...][None, :]
        out_ref[:, at : at + ref.shape[1]] = normed.astype(BF)
    rot = rot_ref[...]
    both = jnp.concatenate([rot, jnp.zeros_like(rot)], axis=1)
    out_ref[:, QLAT + KVLAT : QLAT + KVLAT + 128] = both
    out_ref[:, QLAT + KVLAT + 128 :] = jnp.zeros((rot.shape[0], 128), BF)


def prepare(query_latent, kv_latent, key_rot, query_gain, kv_gain):
    return pl.pallas_call(
        prepare_body,
        out_shape=jax.ShapeDtypeStruct((query_latent.shape[0], LATENT), BF),
        name="prepare",
    )(query_latent, kv_latent, key_rot, query_gain, kv_gain)


def heads_body(*refs):
    blocks = refs[:8]
    key_ref, value_ref, nope_ref, rope_ref, cos_ref, sin_ref = refs[8:14]
    kv_ref, low_ref, high_ref = refs[14:]
    kv = jnp.concatenate([r[:, QLAT : QLAT + KVLAT] for r in blocks], axis=0)
    keys = dot(kv, key_ref[...]).astype(BF)
    values = dot(value_ref[...].T, kv, NT).astype(BF)
    rots = jnp.concatenate(
        [r[:, QLAT + KVLAT : QLAT + KVLAT + 128] for r in blocks], axis=0
    ).astype(F32)
    half = KEYS // 2
    for k in range(2):
        at = k * KEYS
        to = k * PIECE
        pair = rots[at : at + half] + pltpu.roll(rots[at + half : at + KEYS], ROPE, 1)
        kv_ref[to : to + KEYS, :] = keys[at : at + KEYS]
        kv_ref[to + KEYS : to + KEYS + half, :] = pair.astype(BF)
        for c in range(4):
            row = to + KEYS + half + 128 * c
            kv_ref[row : row + 128, :] = values[:, at + 128 * c : at + 128 * (c + 1)]
    query_in = jnp.concatenate([r[:, :QLAT] for r in blocks], axis=0)
    query = dot(jnp.concatenate([nope_ref[...].T, rope_ref[...]], axis=0), query_in, NT)
    first = query[NOPE : NOPE + ROPE // 2]
    second = query[NOPE + ROPE // 2 :]
    cosine = cos_ref[...]
    sine = sin_ref[...]
    rot = jnp.concatenate([first * cosine - second * sine, second * cosine + first * sine], axis=0)
    nope = query[:NOPE].astype(BF)
    rot = rot.astype(BF)
    blank = jnp.zeros_like(rot)
    low_ref[...] = jnp.concatenate([nope, rot, blank], axis=0)
    high_ref[...] = jnp.concatenate([nope, blank, rot], axis=0)


def heads(blocks, key_w, value_w, nope_w, rope_w, cosine, sine):
    rows = 8 * blocks[0].shape[0]
    query = jax.ShapeDtypeStruct((256, rows), BF)
    return pl.pallas_call(
        heads_body,
        out_shape=[jax.ShapeDtypeStruct((2 * PIECE, 128), BF), query, query],
        cost_estimate=pl.CostEstimate(
            flops=2 * rows * (QLAT * 192 + KVLAT * 256), bytes_accessed=6 << 20, transcendentals=0
        ),
        name="heads",
    )(*blocks, key_w, value_w, nope_w, rope_w.T, cosine, sine)


def join_body(a_ref, b_ref, c_ref, d_ref, one_ref, two_ref):
    rows = a_ref.shape[0]
    one_ref[:rows, :] = a_ref[...]
    one_ref[rows:, :] = b_ref[...]
    two_ref[:rows, :] = c_ref[...]
    two_ref[rows:, :] = d_ref[...]


def join(blocks):
    rows = blocks[0].shape[0]
    out = jax.ShapeDtypeStruct((2 * rows, 128), BF)
    return pl.pallas_call(join_body, out_shape=[out] * 2, name="join")(*blocks)


def load_piece(ref, k):
    at = pl.multiple_of(k * PIECE, PIECE)
    half = KEYS // 2
    pair = ref[pl.ds(at + KEYS, half), :]
    left = jnp.concatenate([ref[pl.ds(at, half), :], pair], axis=1)
    right = jnp.concatenate([ref[pl.ds(at + half, half), :], pair], axis=1)
    value = [ref[pl.ds(at + KEYS + half + 128 * c, 128), :] for c in range(4)]
    return left, right, jnp.concatenate(value, axis=1)


def own_body(kpos_ref, qpos_ref, low_ref, high_ref, kv_ref, *refs):
    m_ref, l_ref, acc_ref = refs[-3:]
    tile = 256
    half = KEYS // 2
    pieces = [load_piece(kv_ref, k) for k in range(2)]
    lefts = [pieces[0][0], pieces[0][1], pieces[1][0], pieces[1][1]]
    value = jnp.concatenate([pieces[0][2], pieces[1][2]], axis=1)

    def one(part, _):
        cols = pl.ds(pl.multiple_of(part * tile, tile), tile)
        scores = []
        for k, left in enumerate(lefts):
            s = dot(left, (high_ref if k % 2 else low_ref)[:, cols])
            allowed = kpos_ref[k * half : (k + 1) * half, :] <= qpos_ref[:, cols]
            scores.append(jnp.where(allowed, s, -1e30))
        peaks = [jnp.max(s, axis=0, keepdims=True) for s in scores]
        m = jnp.maximum(jnp.maximum(peaks[0], peaks[1]), jnp.maximum(peaks[2], peaks[3]))
        base = m * SCALE2
        probs = [jnp.exp2(s * SCALE2 - base) for s in scores]
        sums = [jnp.sum(p, axis=0, keepdims=True) for p in probs]
        m_ref[:, cols] = m
        l_ref[:, cols] = (sums[0] + sums[1]) + (sums[2] + sums[3])
        acc_ref[:, cols] = dot(value, jnp.concatenate([p.astype(BF) for p in probs], axis=0))
        return 0

    lax.fori_loop(0, low_ref.shape[1] // tile, one, 0)


def own_attention(low, high, kv, positions):
    rows = low.shape[1]
    thin = jax.ShapeDtypeStruct((1, rows), F32)
    vmem = pl.BlockSpec(memory_space=pltpu.VMEM)
    return pl.pallas_call(
        own_body,
        in_specs=[vmem] * 5,
        out_specs=[vmem] * 3,
        out_shape=[thin, thin, jax.ShapeDtypeStruct((VDIM, rows), F32)],
        cost_estimate=pl.CostEstimate(
            flops=2 * rows * rows * 384, bytes_accessed=4 << 20, transcendentals=rows * rows
        ),
        name="own_attention",
    )(positions.reshape(-1, 1), positions.reshape(1, -1), low, high, kv)


def more_body(arrays, first, final, flags_ref, low_ref, high_ref, *refs):
    pieces = refs[:arrays]
    m_in, l_in, acc_in = refs[arrays : arrays + 3]
    keys_ref, sems = refs[-2:]
    m_ref, l_ref, acc_ref = refs[-5:-2]
    size = pieces[0].shape[0]

    def fetch(ref, number):
        target = keys_ref.at[pl.ds(pl.multiple_of(number * size, size), size)]
        return pltpu.make_async_copy(ref, target, sems.at[number])

    for number, ref in enumerate(pieces):
        fetch(ref, number).start()
    tile = 256
    tiles = low_ref.shape[1] // tile

    def start():
        m_ref[...] = m_in[...]
        l_ref[...] = l_in[...]
        acc_ref[...] = acc_in[...]

    def score(piece, t):
        cols = slice(t * tile, (t + 1) * tile)
        return dot(piece[0], low_ref[:, cols]), dot(piece[1], high_ref[:, cols])

    def over(step, wait):
        def array(number, _):
            if wait:
                fetch(pieces[0], number).wait()

            def one(k, _):
                @pl.when(flags_ref[first + 2 * number + k] != 0)
                def _():
                    step(2 * number + k)

                return 0

            lax.fori_loop(0, 2, one, 0)
            return 0

        lax.fori_loop(0, arrays, array, 0)

    def weigh(s, t):
        cols = slice(t * tile, (t + 1) * tile)
        base = m_ref[:, cols] * SCALE2
        p = jnp.exp2(s[0] * SCALE2 - base)
        q = jnp.exp2(s[1] * SCALE2 - base)
        l_ref[:, cols] += jnp.sum(p, axis=0, keepdims=True) + jnp.sum(q, axis=0, keepdims=True)
        return jnp.concatenate([p.astype(BF), q.astype(BF)], axis=0)

    def gather(piece, probs, t):
        cols = slice(t * tile, (t + 1) * tile)
        acc_ref[:, cols] += dot(piece[2], probs)

    def quick(k):
        block = [load_piece(keys_ref, 2 * k), load_piece(keys_ref, 2 * k + 1)]
        steps = [(piece, t) for piece in block for t in range(tiles)]
        s = score(*steps[0])
        before = None
        for i, (_, t) in enumerate(steps):
            after = score(*steps[i + 1]) if i + 1 < len(steps) else None
            if before is not None:
                gather(steps[i - 1][0], before, steps[i - 1][1])
            before = weigh(s, t)
            s = after
        gather(steps[-1][0], before, steps[-1][1])

    def careful(k):
        def one(i, _):
            piece = load_piece(keys_ref, 2 * k + i // tiles)
            cols = pl.ds(pl.multiple_of((i % tiles) * tile, tile), tile)
            p = dot(piece[0], low_ref[:, cols])
            q = dot(piece[1], high_ref[:, cols])
            before = m_ref[:, cols]
            peak = jnp.maximum(jnp.max(p, axis=0, keepdims=True), jnp.max(q, axis=0, keepdims=True))
            m = jnp.maximum(before, peak)
            alpha = jnp.exp2((before - m) * SCALE2)
            p = jnp.exp2(p * SCALE2 - m * SCALE2)
            q = jnp.exp2(q * SCALE2 - m * SCALE2)
            m_ref[:, cols] = m
            total = jnp.sum(p, axis=0, keepdims=True) + jnp.sum(q, axis=0, keepdims=True)
            l_ref[:, cols] = l_ref[:, cols] * alpha + total
            probs = jnp.concatenate([p.astype(BF), q.astype(BF)], axis=0)
            acc_ref[:, cols] = acc_ref[:, cols] * alpha + dot(piece[2], probs)
            return 0

        lax.fori_loop(0, 2 * tiles, one, 0)

    start()
    over(quick, True)
    safe = jnp.where(l_ref[...] < LIMIT, 0.0, 1.0)

    @pl.when(jnp.max(safe) > 0.0)
    def _():
        start()
        over(careful, False)

    if final:
        done = (acc_ref[...] / l_ref[...]).astype(BF)
        for b in range(4):
            refs[arrays + 3 + b][...] = done[:, 256 * b : 256 * (b + 1)]


def more_attention(low, high, arrays, flags, first, state, final=False):
    rows = low.shape[1]
    keys = 4 * len(arrays) * KEYS
    shapes = [(1, rows), (1, rows), (VDIM, rows)]
    if final:
        out_shape = [jax.ShapeDtypeStruct((VDIM, rows // 4), BF)] * 4
        scratch = [pltpu.VMEM(s, F32) for s in shapes]
    else:
        out_shape = [jax.ShapeDtypeStruct(s, F32) for s in shapes]
        scratch = []
    vmem = pl.BlockSpec(memory_space=pltpu.VMEM)
    count = len(arrays)
    scratch += [
        pltpu.VMEM((count * arrays[0].shape[0], 128), BF),
        pltpu.SemaphoreType.DMA((count,)),
    ]
    return pl.pallas_call(
        functools.partial(more_body, count, first, final),
        in_specs=[pl.BlockSpec(memory_space=pltpu.SMEM), vmem, vmem]
        + [pl.BlockSpec(memory_space=pl.ANY)] * count
        + [vmem] * 3,
        out_specs=[vmem] * len(out_shape),
        out_shape=out_shape,
        scratch_shapes=scratch,
        cost_estimate=pl.CostEstimate(
            flops=rows * keys * 384, bytes_accessed=4 << 20, transcendentals=rows * keys
        ),
        name="more_attention",
    )(flags, low, high, *arrays, *state)


def project_body(*refs):
    left = jnp.concatenate([r[...] for r in refs[:4]], axis=0)
    right = jnp.concatenate([r[...] for r in refs[4:8]], axis=0)
    mine, other = refs[8:]
    result = dot(left, right, (((0,), (0,)), ((), ())))
    rows = mine.shape[0]
    mine[...] = result[:rows]
    other[...] = result[rows:].astype(BF)


def project(attended, blocks):
    rows = attended[0].shape[1] // 2
    width = blocks[0].shape[1]
    return pl.pallas_call(
        project_body,
        grid=(width // 512,),
        in_specs=[whole(a.shape) for a in attended] + [columns(128)] * 4,
        out_specs=[columns(rows)] * 2,
        out_shape=[
            jax.ShapeDtypeStruct((rows, width), F32),
            jax.ShapeDtypeStruct((rows, width), BF),
        ],
        name="project",
    )(*attended, *blocks)


def angles(positions):
    half = ROPE // 2
    freq = 1.0 / THETA ** (jnp.arange(half, dtype=F32) * 2.0 / ROPE)
    return positions.astype(F32), freq


def turn(values):
    half = ROPE // 2
    return jnp.concatenate([-values[:, half:], values[:, :half]], axis=-1)


LINE = (0, 1, -1, 2)


def sources():
    near = [(d, 0) for d in LINE]
    wide = [(a, 1) for a in LINE[:2]] + [(a, -1) for a in LINE[2:]]
    more = [(a, 1) for a in LINE[2:]] + [(a, -1) for a in LINE[:2]]
    far = [(a, 2) for a in LINE]
    return near + wide + more + far


def own_block(query_latent, kv_latent, rope_key, query_gain, kv_gain):
    local = query_latent.shape[0]
    first = (lax.axis_index("ep") * 8 + lax.axis_index("tp")) * local
    place, freq = angles(first + jnp.arange(local, dtype=jnp.int32))
    angle = place[:, None] * freq[None, :]
    angle = jnp.concatenate([angle, angle], axis=-1)
    key_in = rope_key.astype(F32)
    key_rot = (key_in * jnp.cos(angle) + turn(key_in) * jnp.sin(angle)).astype(BF)
    return prepare(query_latent, kv_latent, key_rot, query_gain, kv_gain)


def mixer(query_latent, query_nope_w, query_rope_w, key_up_w, value_up_w, output_w, block):
    local = query_latent.shape[0]
    group = local * 8
    ep = lax.axis_index("ep")
    tp = lax.axis_index("tp")
    z, x = ep // 4, ep % 4
    y, core = tp // 2, tp % 2
    behind, ahead, far = ring(block, along_y)
    outputs = (output_w, *ring(output_w, along_y))
    blocks = [block, swap(block), behind, swap(ahead), ahead, swap(behind), far, swap(far)]
    turned = 1 - 2 * core
    chips = (y + turned * np.array([0, -1, 1, 2], np.int32)) % 4
    one = np.array([s[0] for s in sources()], np.int32)
    two = np.array([s[1] for s in sources()], np.int32)
    dz = jnp.where(core == 0, one, two)
    dx = jnp.where(core == 0, two, one)
    flags = (((z - dz) % 4) * 4 + (x - dx) % 4 < ep).astype(jnp.int32)
    order = chips[:, None] * 2 + (core ^ np.array([[0, 1]], np.int32))
    inside = (order.reshape(8, 1) * local + np.arange(local, dtype=np.int32)[None, :]).reshape(-1)
    place, freq = angles(ep * group + inside)
    angle = freq[:, None] * place[None, :]
    turns = jnp.cos(angle), jnp.sin(angle)
    kv, low, high = heads(blocks, key_up_w, value_up_w, query_nope_w, query_rope_w, *turns)
    one, two = join([kv, *ring(kv, along_one)])
    behind, ahead, far = ring_halves(one, two, along_two)
    state = own_attention(low, high, kv, inside)
    state = more_attention(low, high, (one, two), flags, 0, state)
    wide = behind[0], ahead[1]
    rest = behind[1], ahead[0], *far
    state = more_attention(low, high, wide, flags, 4, state)
    attended = more_attention(low, high, rest, flags, 8, state, final=True)
    attended = (
        attended[0],
        send(attended[2], along_y(1)),
        send(attended[1], along_y(-1)),
        send(attended[3], along_y(2)),
    )
    mine, other = project(attended, outputs)
    return add((mine, swap(other)))[0]


def per_device(
    query_latent,
    kv_latent,
    rope_key,
    query_gain,
    kv_gain,
    query_nope_w,
    query_rope_w,
    key_up_w,
    value_up_w,
    output_w,
    expert_in,
    moe_gain,
    routes,
    route_weight,
    gate_w,
    up_w,
    down_w,
):
    block = own_block(query_latent, kv_latent, rope_key, query_gain, kv_gain)
    mixer_out = mixer(
        query_latent, query_nope_w, query_rope_w, key_up_w, value_up_w, output_w, block
    )
    expert_out = experts_half(
        expert_in, moe_gain, routes, route_weight, gate_w, up_w, down_w
    )
    return (mixer_out, expert_out)


def solution(mesh):
    placed = (
        P(("ep", "tp"), None),
        P(("ep", "tp"), None),
        P(("ep", "tp"), None),
        P(),
        P(),
        P(None, "tp"),
        P(None, "tp"),
        P(None, "tp"),
        P(None, "tp"),
        P("tp", None),
        P(("ep", "tp"), None),
        P(),
        P(("ep", "tp"), None),
        P(("ep", "tp"), None),
        P("ep", None, "tp"),
        P("ep", None, "tp"),
        P("ep", "tp", None),
    )
    return jax.shard_map(
        per_device,
        mesh=mesh,
        in_specs=placed,
        out_specs=(P(("ep", "tp"), None), P(("ep", "tp"), None)),
        check_vma=False,
    )
```
